256 devices in a mesh: ep: 64 (over z, y, core), tp: 4 (over x).
Axes of the slice: x: 4, y: 4, z: 8, core: 2. Of those that a mesh axis runs over, the one named last changes fastest.
Arguments:
- mixer_input: bfloat16 [32768, 2048], P('ep'), may hold values from -6 to 6
- mixer_gain: bfloat16 [2048], replicated, may hold values from 0.099609375 to 1.8984375
- pool_in: bfloat16 [2048, 1024], P(None, 'tp'), may hold values from -0.125 to 0.125
- pool_map: bfloat16 [4, 256, 256], P('tp'), may hold values from -0.375 to 0.375
- pool_scale: bfloat16 [1024], P('tp'), may hold values from 0.099609375 to 1.8984375
- pool_out: bfloat16 [1024, 2048], P('tp'), may hold values from -0.1875 to 0.1875
- expert_input: bfloat16 [24576, 2048], P('ep'), may hold values from -6 to 6
- expert_gain: bfloat16 [2048], replicated, may hold values from 0.099609375 to 1.8984375
- group_router: bfloat16 [2048, 4], replicated, may hold values from -0.125 to 0.125
- expert_router: bfloat16 [2048, 64], replicated, may hold values from -0.125 to 0.125
- routes: int32 [24576, 2], P('ep'), may hold values from 0 to 63, all different within a row; in each aligned block of 96 rows (0 to 95, 96 to 191, ...) at most 6 rows name the same one
- gate_weight: bfloat16 [64, 2048, 1024], P('ep', None, 'tp'), may hold values from -0.125 to 0.125
- up_weight: bfloat16 [64, 2048, 1024], P('ep', None, 'tp'), may hold values from -0.125 to 0.125
- down_weight: bfloat16 [64, 1024, 2048], P('ep', 'tp'), may hold values from -0.1875 to 0.1875
Outputs:
- mixer_output: bfloat16 [32768, 2048], P(('ep', 'tp'))
- expert_output: bfloat16 [24576, 2048], P(('ep', 'tp'))
The draws below stay inside these ranges and needn't reach their ends.
Inputs may be any that keep to these rules, and one draw needn't show every extreme that they name: `routes`: each row names two different experts. In each aligned block of 96 rows no expert is named more than 6 times, a bound that some block reaches.
All inputs are finite; a program needn't handle non-finite values.
Results may differ from the reference program's by a relative error of at most 0.01.
Values may be sent and summed in bfloat16 or wider, within the bound.
No kernel may reach another device: no remote copies, remote signals or barrier semaphores. Data moves between devices by JAX's collectives and lax.ppermute only.
A program may use at most 64 MiB of HBM per device.

```python
import math
import jax
import jax.numpy as jnp
import numpy as np
from jax import lax

D = 2048
MIX_A = 1024
POOL_GROUPS = 4
POOL_CH = 256
RIM = 15
HID = 1024
EXPERT_GROUPS = 4
EXPERTS = 64
TOK_A = 32768
TB_DEV = 96
TOK_B = 24576
CAPQ = 6
N_TP = 4


def levels(stream_key, extent, shards, least, largest):
    loudness, own = 1.0, jax.random.fold_in(stream_key, 6)
    for dim, parts in shards:
        draws = jnp.exp(jax.random.uniform(jax.random.fold_in(own, dim), (parts,), jnp.float32, least / len(shards), largest / len(shards)))
        loudness = loudness * jnp.repeat(draws, extent[dim] // parts).reshape([-1 if axis == dim else 1 for axis in range(len(extent))])
    return loudness


def shared_out(own_key, own, number, rows, number_of, top, bound, lean):
    order = jax.random.permutation(own_key, number_of)
    crowded, usual = portions_of(number_of, rows * top, bound, lean, True), portions_of(number_of, rows * top, bound, lean, False)
    places = jnp.arange(number_of)

    def named(lengths, turn):
        used = int((lengths > 0).sum())
        fixed = max(1, used // 4)
        shifted = fixed + (places - fixed + turn * (used - fixed)) % max(1, number_of - fixed)
        return jnp.zeros((number_of,), jnp.int32).at[order[jnp.where(places < fixed, places, shifted)]].set(jnp.asarray(lengths, jnp.int32))

    lengths = jnp.where(number % 4 == 0, named(crowded, number // 4), named(usual, number - number // 4 - 1))
    mixed = jax.random.permutation(jax.random.fold_in(own, 3), number_of)
    giver, sink = mixed[0:number_of // 2 * 2:2], mixed[1:number_of // 2 * 2:2]
    room = jnp.minimum(lengths[giver] - 1, bound - lengths[sink]) // 2
    room = jnp.where((giver == order[0]) | (sink == order[0]) | (lengths[sink] == 0), 0, jnp.maximum(room, 0))
    shifted = jax.random.randint(jax.random.fold_in(own, 4), (number_of // 2,), 0, 1 << 20) % (room + 1)
    lengths = lengths.at[giver].add(-shifted).at[sink].add(shifted)
    labels = jnp.searchsorted(jnp.cumsum(lengths), jnp.arange(rows * top), side="right").astype(jnp.int32)
    grid = labels.reshape(top, rows).T
    grid = grid[jax.random.permutation(jax.random.fold_in(own, 1), rows)]
    turn = jax.random.randint(jax.random.fold_in(own, 2), (rows, 1), 0, top)
    return jnp.take_along_axis(grid, (jnp.arange(top)[None, :] + turn) % top, axis=1)


def portions_of(number_of, total, most, lean, full):
    loads = [(1 << 20) // math.isqrt(grade ** lean) + 1 for grade in range(1, number_of + 1)]
    largest = most if full else min(most, max(-(-total // number_of), total * loads[0] // sum(loads)))
    least = 1 if total - largest >= number_of - 1 else 0
    holding, spare = [largest] + [least] * (number_of - 1), total - largest - least * (number_of - 1)
    while spare > 0:
        movable = [i for i in range(1, number_of) if holding[i] < largest] or [i for i in range(1, number_of) if holding[i] < most]
        mass, budget = sum([loads[i] for i in movable]), spare
        for i in movable:
            more = min(most - holding[i], max(1, budget * loads[i] // mass), spare)
            holding[i] = holding[i] + more
            spare = spare - more
    return np.array(holding)


def normal_values(key, extent, spread, most, shards=(), held_as=jnp.bfloat16):
    entries = spread * jax.random.normal(key, extent, jnp.float32)
    if shards:
        entries = entries * levels(key, extent, shards, -0.22, 0.18)
    return jnp.clip(entries, -most, most).astype(held_as)


def setup_inputs(seed: int = 0) -> dict:
    key_of = jax.random.split(jax.random.key(seed), 15)
    mixer_input = normal_values(key_of[0], (TOK_A, D), 1.0, 6.0, ((0, 64),))
    mixer_gain = jnp.clip(1.0 + 0.18 * jax.random.normal(key_of[1], (D,), jnp.float32), 0.099609375, 1.8984375).astype(jnp.bfloat16)
    pool_in = normal_values(key_of[2], (D, MIX_A), D ** -0.5, 0.125, ((1, 4),))
    pool_map = normal_values(key_of[3], (POOL_GROUPS, POOL_CH, POOL_CH), POOL_CH ** -0.5, 0.375, ((0, 4),))
    pool_scale = jnp.clip(1.0 + 0.18 * jax.random.normal(key_of[4], (MIX_A,), jnp.float32), 0.099609375, 1.8984375).astype(jnp.bfloat16)
    pool_out = normal_values(key_of[5], (MIX_A, D), MIX_A ** -0.5, 0.1875, ((0, 4),))
    expert_input = normal_values(key_of[6], (TOK_B, D), 1.0, 6.0, ((0, 64),))
    expert_gain = jnp.clip(1.0 + 0.18 * jax.random.normal(key_of[7], (D,), jnp.float32), 0.099609375, 1.8984375).astype(jnp.bfloat16)
    group_router = normal_values(key_of[8], (D, EXPERT_GROUPS), D ** -0.5, 0.125)
    expert_router = normal_values(key_of[9], (D, EXPERTS), D ** -0.5, 0.125)
    routes_keys = jax.random.split(jax.random.fold_in(key_of[10], 1), TOK_B // TB_DEV)
    routes_turns = jax.random.permutation(jax.random.fold_in(key_of[10], 3), TOK_B // TB_DEV)
    routes = jax.vmap(lambda own, number: shared_out(jax.random.fold_in(key_of[10], 2), own, number, TB_DEV, EXPERTS, 2, CAPQ, 2))(routes_keys, routes_turns).reshape((TOK_B, 2))
    gate_weight = normal_values(key_of[11], (EXPERTS, D, HID), D ** -0.5, 0.125, ((0, 64), (2, 4)))
    up_weight = normal_values(key_of[12], (EXPERTS, D, HID), D ** -0.5, 0.125, ((0, 64), (2, 4)))
    down_weight = normal_values(key_of[13], (EXPERTS, HID, D), HID ** -0.5, 0.1875, ((0, 64), (1, 4)))
    return {"mixer_input": mixer_input, "mixer_gain": mixer_gain, "pool_in": pool_in, "pool_map": pool_map, "pool_scale": pool_scale, "pool_out": pool_out, "expert_input": expert_input, "expert_gain": expert_gain, "group_router": group_router, "expert_router": expert_router, "routes": routes, "gate_weight": gate_weight, "up_weight": up_weight, "down_weight": down_weight}


EPS = 1e-06
block_rows = 128

def norm_rows(values, gain):
    floats = values.astype(jnp.float32)
    scale = lax.rsqrt(lax.optimization_barrier(jnp.mean(floats * floats, axis=-1, keepdims=True)) + EPS)
    return (floats * scale * gain.astype(jnp.float32)).astype(jnp.bfloat16)

def route_weights(rows, group_router, expert_router, route_rows):
    group_logits = jnp.dot(rows, group_router, preferred_element_type=jnp.float32)
    expert_logits = jnp.dot(rows, expert_router, preferred_element_type=jnp.float32)
    groups = group_logits.shape[1]
    experts = expert_logits.shape[1]
    member = (jnp.arange(experts, dtype=jnp.int32)[:, None] // (experts // groups) == jnp.arange(groups, dtype=jnp.int32)[None, :]).astype(jnp.float32)
    group_exp = jnp.exp(group_logits)
    group_prob = group_exp / lax.optimization_barrier(jnp.sum(group_exp, axis=1, keepdims=True))
    expert_exp = jnp.exp(expert_logits)
    within = jnp.dot(expert_exp, member, precision=lax.Precision.HIGHEST)
    prob = expert_exp * jnp.dot(group_prob / within, member.T, precision=lax.Precision.HIGHEST)
    chosen = (route_rows[:, :, None] == jnp.arange(experts, dtype=jnp.int32)[None, None, :]).astype(jnp.float32)
    picked = lax.optimization_barrier(jnp.sum(chosen * prob[:, None, :], axis=2))
    return picked / lax.optimization_barrier(jnp.sum(picked, axis=1, keepdims=True))

def reference(mixer_input, mixer_gain, pool_in, pool_map, pool_scale, pool_out, expert_input, expert_gain, group_router, expert_router, routes, gate_weight, up_weight, down_weight):
    normed = norm_rows(mixer_input, mixer_gain)
    pooled_in = jnp.dot(normed, pool_in, preferred_element_type=jnp.float32).astype(jnp.bfloat16)
    tokens = pooled_in.shape[0]
    floats = pooled_in.astype(jnp.float32).reshape(tokens, POOL_GROUPS, POOL_CH)
    padded = jnp.concatenate([jnp.zeros((RIM, POOL_GROUPS, POOL_CH), jnp.float32), floats], axis=0)
    position = jnp.arange(tokens, dtype=jnp.int32)
    group_list = []
    for group in range(POOL_GROUPS):
        window = 2 ** (group + 1)
        window_sum = jnp.zeros((tokens, POOL_CH), jnp.float32)
        for offset in range(window):
            window_sum = window_sum + padded[RIM - offset:RIM - offset + tokens, group]
        counts = jnp.minimum(position + 1, window).astype(jnp.float32)
        group_list.append(window_sum / counts[:, None] - floats[:, group])
    pooled = jnp.stack(group_list, axis=1).astype(jnp.bfloat16)
    mapped = jnp.einsum('tgc,gce->tge', pooled.astype(jnp.float32), pool_map.astype(jnp.float32))
    mixed = (mapped.reshape(tokens, MIX_A) * pool_scale.astype(jnp.float32)).astype(jnp.bfloat16)
    quarter = MIX_A // N_TP
    mixer_sum = jnp.zeros((tokens, D), jnp.float32)
    for part in range(N_TP):
        partial_value = jnp.dot(mixed[:, part * quarter:(part + 1) * quarter], pool_out[part * quarter:(part + 1) * quarter], preferred_element_type=jnp.float32).astype(jnp.bfloat16)
        partial_value = lax.optimization_barrier(partial_value)
        mixer_sum = mixer_sum + partial_value.astype(jnp.float32)
    mixer_output = mixer_sum.astype(jnp.bfloat16)
    normed_exp = norm_rows(expert_input, expert_gain)
    weights = route_weights(normed_exp, group_router, expert_router, routes)
    tokens_b = normed_exp.shape[0]
    flat = routes.reshape(-1).astype(jnp.int32)
    assigned = flat.shape[0]
    owner = (jnp.arange(assigned, dtype=jnp.int32) // 2).astype(jnp.int32)
    order = jnp.argsort(flat, stable=True).astype(jnp.int32)
    sorted_expert = flat[order]
    sorted_owner = owner[order]
    counts_all = lax.optimization_barrier(jnp.sum((flat[:, None] == jnp.arange(EXPERTS, dtype=jnp.int32)[None, :]).astype(jnp.int32), axis=0))
    starts = (jnp.cumsum(counts_all) - counts_all).astype(jnp.int32)
    padded_counts = (counts_all + block_rows - 1) // block_rows * block_rows
    pad_starts = (jnp.cumsum(padded_counts) - padded_counts).astype(jnp.int32)
    pad_ends = pad_starts + padded_counts
    dest = (pad_starts[sorted_expert] + jnp.arange(assigned, dtype=jnp.int32) - starts[sorted_expert]).astype(jnp.int32)
    blocks = (assigned + EXPERTS * (block_rows - 1) + block_rows - 1) // block_rows
    buffer = jnp.zeros((blocks * block_rows, D), jnp.bfloat16).at[dest].set(normed_exp[sorted_owner])
    block_start = jnp.arange(blocks, dtype=jnp.int32) * block_rows
    block_expert = jnp.clip(lax.optimization_barrier(jnp.sum((pad_ends[None, :] <= block_start[:, None]).astype(jnp.int32), axis=1)), 0, EXPERTS - 1).astype(jnp.int32)
    hid_part = HID // N_TP

    def expert_block(pair):
        rows_here, expert = pair
        gate = jnp.dot(rows_here, gate_weight[expert], preferred_element_type=jnp.float32)
        upward = jnp.dot(rows_here, up_weight[expert], preferred_element_type=jnp.float32)
        hidden = (jax.nn.silu(gate) * upward).astype(jnp.bfloat16)
        result = jnp.zeros((block_rows, D), jnp.float32)
        for part in range(N_TP):
            partial_value = jnp.dot(hidden[:, part * hid_part:(part + 1) * hid_part], down_weight[expert, part * hid_part:(part + 1) * hid_part], preferred_element_type=jnp.float32).astype(jnp.bfloat16)
            partial_value = lax.optimization_barrier(partial_value)
            result = result + partial_value.astype(jnp.float32)
        return result.astype(jnp.bfloat16)
    results = lax.map(expert_block, (buffer.reshape(blocks, block_rows, D), block_expert)).reshape(-1, D)
    per_copy = results[dest].astype(jnp.float32)
    copy_weight = weights.reshape(-1)[order]
    expert_sum = jnp.zeros((tokens_b, D), jnp.float32).at[sorted_owner].add(per_copy * copy_weight[:, None])
    return (mixer_output, expert_sum.astype(jnp.bfloat16))
```

```python
import jax
import jax.numpy as jnp
from jax import lax
from jax.experimental import pallas as pl
from jax.sharding import PartitionSpec as P


RIM = 15
EPS = 1e-06
CHUNKS = 1
WIDTHS = (1024, 1024)


def passed_along(value, axis, steps):
    count = lax.axis_size(axis)
    leading, last = (max(0, -steps), min(count, count - steps))
    return lax.ppermute(value, axis, [(source, source + steps) for source in range(leading, last)])


def swapped(value, mask):
    count = lax.axis_size("tp")
    return lax.ppermute(value, "tp", [(source, source ^ mask) for source in range(count)])


def norm_rows(values, gain):
    floats = values.astype(jnp.float32)
    scale = lax.rsqrt(jnp.mean(floats * floats, axis=-1, keepdims=True) + EPS)
    return (floats * scale * gain.astype(jnp.float32)).astype(jnp.bfloat16)


def mixer_partial(mixer_input, mixer_gain, pool_in, pool_map, pool_scale, pool_out):
    normed = norm_rows(mixer_input, mixer_gain)
    pooled_in = jnp.dot(normed, pool_in, preferred_element_type=jnp.float32).astype(jnp.bfloat16)
    local_rows = pooled_in.shape[0]
    groups_here = pool_map.shape[0]
    channels = pool_map.shape[1]
    border = passed_along(pooled_in[local_rows - RIM :], "ep", 1)
    padded = jnp.concatenate([border, pooled_in], axis=0).astype(jnp.float32)
    padded = padded.reshape(local_rows + RIM, groups_here, channels)
    leading = lax.axis_index("tp") * groups_here
    windows = jnp.left_shift(jnp.int32(2), leading + jnp.arange(groups_here, dtype=jnp.int32))
    window_sum = jnp.zeros((local_rows, groups_here, channels), jnp.float32)
    for offset in range(RIM + 1):
        active = (offset < windows).astype(jnp.float32)
        window_sum = (
            window_sum + padded[RIM - offset : RIM - offset + local_rows] * active[None, :, None]
        )
    position = lax.axis_index("ep") * local_rows + jnp.arange(local_rows, dtype=jnp.int32)
    counts_here = jnp.minimum(position[:, None] + 1, windows[None, :]).astype(jnp.float32)
    pooled = (window_sum / counts_here[:, :, None] - padded[RIM:]).astype(jnp.bfloat16)
    mapped = jnp.einsum("tgc,gce->tge", pooled, pool_map, preferred_element_type=jnp.float32)
    mixed_rows = (
        mapped.reshape(local_rows, groups_here * channels) * pool_scale.astype(jnp.float32)
    ).astype(jnp.bfloat16)
    return jnp.dot(mixed_rows, pool_out, preferred_element_type=jnp.float32).astype(jnp.bfloat16)


def mixer_reduce(partial_rows):
    count = lax.axis_size("tp")
    place = lax.axis_index("tp")
    rows = partial_rows.shape[0] // count

    def piece(k):
        return lax.dynamic_slice_in_dim(partial_rows, (place ^ k) * rows, rows, 0)

    total = piece(0).astype(jnp.float32)
    for k in range(1, count):
        total = total + swapped(piece(k), k).astype(jnp.float32)
    return total.astype(jnp.bfloat16)


def dispatch_kernel(x_ref, gain_ref, routes_ref, *outs):
    normed_ref, pick_ref = outs[0], outs[1]
    payloads = outs[2:]
    tokens = x_ref.shape[0]
    floats = x_ref[...].astype(jnp.float32)
    scale = lax.rsqrt(jnp.mean(floats * floats, axis=-1, keepdims=True) + EPS)
    normed = (floats * scale * gain_ref[...].astype(jnp.float32)).astype(jnp.bfloat16)
    normed_ref[...] = normed
    routes = routes_ref[...]
    slots = pick_ref.shape[2]
    experts = 64
    each = slots // experts
    expert = lax.broadcasted_iota(jnp.int32, (tokens, experts), 1)
    first = routes[:, 0:1] == expert
    second = routes[:, 1:2] == expert
    named = jnp.where(first | second, 1.0, 0.0)
    earlier = lax.broadcasted_iota(jnp.int32, (tokens, tokens), 1) < lax.broadcasted_iota(
        jnp.int32, (tokens, tokens), 0
    )
    before = jnp.dot(
        jnp.where(earlier, 1.0, 0.0).astype(jnp.bfloat16),
        named.astype(jnp.bfloat16),
        preferred_element_type=jnp.float32,
    )
    spread = lax.broadcasted_iota(jnp.int32, (experts, slots), 1) // each == lax.broadcasted_iota(
        jnp.int32, (experts, slots), 0
    )
    spread = jnp.where(spread, 1.0, 0.0).astype(jnp.bfloat16)
    within = (lax.broadcasted_iota(jnp.int32, (tokens, slots), 1) % each).astype(jnp.float32)
    chosen = []
    for mask in (first, second):
        place = jnp.where(mask, before, -1.0).astype(jnp.bfloat16)
        spread_place = jnp.dot(place, spread, preferred_element_type=jnp.float32)
        chosen.append(jnp.where(spread_place == within, 1.0, 0.0))
    pick_ref[0] = chosen[0].astype(jnp.bfloat16)
    pick_ref[1] = chosen[1].astype(jnp.bfloat16)
    either = (chosen[0] + chosen[1]).astype(jnp.bfloat16)
    for index, out in enumerate(payloads):
        width = out.shape[1]
        out[...] = lax.dot_general(
            either,
            normed[:, index * width : (index + 1) * width],
            (((0,), (0,)), ((), ())),
            preferred_element_type=jnp.float32,
        ).astype(jnp.bfloat16)


def dispatch(x, gain, routes, experts, slots_each):
    tokens, model = x.shape
    slots = experts * slots_each
    return pl.pallas_call(
        dispatch_kernel,
        out_shape=[
            jax.ShapeDtypeStruct((tokens, model), jnp.bfloat16),
            jax.ShapeDtypeStruct((2, tokens, slots), jnp.bfloat16),
        ]
        + [jax.ShapeDtypeStruct((slots, model // CHUNKS), jnp.bfloat16)] * CHUNKS,
        name="dispatch",
    )(x, gain.reshape(1, model), routes)


def route_weights(rows, group_router, expert_router, route_rows):
    group_logits = jnp.dot(rows, group_router, preferred_element_type=jnp.float32)
    expert_logits = jnp.dot(rows, expert_router, preferred_element_type=jnp.float32)
    groups = group_logits.shape[1]
    experts = expert_logits.shape[1]
    member = (
        jnp.arange(experts, dtype=jnp.int32)[:, None] // (experts // groups)
        == jnp.arange(groups, dtype=jnp.int32)[None, :]
    ).astype(jnp.float32)
    group_exp = jnp.exp(group_logits)
    group_prob = group_exp / jnp.sum(group_exp, axis=1, keepdims=True)
    expert_exp = jnp.exp(expert_logits)
    within = jnp.dot(expert_exp, member, precision=lax.Precision.HIGHEST)
    prob = expert_exp * jnp.dot(group_prob / within, member.T, precision=lax.Precision.HIGHEST)
    chosen = (route_rows[:, :, None] == jnp.arange(experts, dtype=jnp.int32)[None, None, :]).astype(
        jnp.float32
    )
    picked = jnp.sum(chosen * prob[:, None, :], axis=2)
    return picked / jnp.sum(picked, axis=1, keepdims=True)


def combine_kernel(returned_ref, pick_ref, weight_ref, *refs):
    out_ref = refs[-1]
    returned = returned_ref[...]
    weight = weight_ref[...]
    total = jnp.dot(pick_ref[0], returned, preferred_element_type=jnp.float32) * weight[:, 0:1]
    total = total + jnp.dot(pick_ref[1], returned, preferred_element_type=jnp.float32) * weight[:, 1:2]
    out_ref[...] = total.astype(jnp.bfloat16)


def combine(returned, pick, weight, index, so_far):
    width = returned.shape[1]
    tokens = pick.shape[1]
    whole = [
        pl.BlockSpec(array.shape, lambda i, n=array.ndim: (0,) * n)
        for array in (returned, pick, weight)
    ]
    extra = [] if so_far is None else [so_far]
    return pl.pallas_call(
        combine_kernel,
        grid=(1,),
        in_specs=whole + [pl.BlockSpec(memory_space=pl.ANY)] * len(extra),
        out_specs=pl.BlockSpec((tokens, width), lambda i: (0, index)),
        out_shape=jax.ShapeDtypeStruct((tokens, sum(WIDTHS)), jnp.bfloat16),
        input_output_aliases={3: 0} if extra else {},
        name="combine",
    )(returned, pick, weight, *extra)


def hidden_kernel(rows_ref, *refs):
    gate_refs, up_refs, out_ref = refs[: len(refs) // 2], refs[len(refs) // 2 : -1], refs[-1]

    def product(parts):
        total, start = None, 0
        for part in parts:
            depth = part.shape[0]
            piece = jnp.dot(
                rows_ref[:, start : start + depth], part[...], preferred_element_type=jnp.float32
            )
            start += depth
            total = piece if total is None else total + piece
        return total

    gate = product(gate_refs)
    out_ref[...] = (gate / (1.0 + jnp.exp(-gate)) * product(up_refs)).astype(jnp.bfloat16)


def hidden_of(rows, gate_parts, up_parts):
    units = gate_parts[0].shape[1]
    return pl.pallas_call(
        hidden_kernel,
        out_shape=jax.ShapeDtypeStruct((rows.shape[0], units), jnp.bfloat16),
        cost_estimate=pl.CostEstimate(
            flops=4 * rows.shape[0] * rows.shape[1] * units, bytes_accessed=4 << 20, transcendentals=0
        ),
        name="hidden",
    )(rows, *gate_parts, *up_parts)


def down_kernel(hidden_refs, down_refs, base_ref, out_ref):
    total = None if base_ref is None else base_ref[...]
    index, start = 0, 0
    for part in down_refs:
        depth = part.shape[0]
        piece = jnp.dot(
            hidden_refs[index][:, start : start + depth],
            part[...],
            preferred_element_type=jnp.float32,
        )
        total = piece if total is None else total + piece
        start += depth
        if start == hidden_refs[index].shape[1]:
            index, start = index + 1, 0
    out_ref[...] = total.astype(out_ref.dtype)


def down_of(hidden, parts, base, dtype):
    rows, width = hidden[0].shape[0], parts[0].shape[1]
    depth = sum(part.shape[0] for part in parts)
    bases = [] if base is None else [base]

    def kernel(*refs):
        refs = list(refs)
        hidden_refs, rest = refs[: len(hidden)], refs[len(hidden) :]
        down_refs, rest = rest[: len(parts)], rest[len(parts) :]
        down_kernel(hidden_refs, down_refs, rest[0] if bases else None, rest[-1])

    return pl.pallas_call(
        kernel,
        out_shape=jax.ShapeDtypeStruct((rows, width), dtype),
        cost_estimate=pl.CostEstimate(
            flops=2 * rows * depth * width, bytes_accessed=4 << 20, transcendentals=0
        ),
        name="down",
    )(*hidden, *parts, *bases)


def exchange(rows, experts):
    slots, width = rows.shape
    each = slots // experts
    moved = lax.all_to_all(
        rows.reshape(experts, each // 2, 2, width), "ep", split_axis=0, concat_axis=0, tiled=True
    )
    return moved.reshape(slots, width)


def layer(
    mixer_input,
    mixer_gain,
    pool_in,
    pool_map,
    pool_scale,
    pool_out,
    expert_input,
    expert_gain,
    group_router,
    expert_router,
    routes,
    gate_weight,
    up_weight,
    down_weight,
):
    tp_count = lax.axis_size("tp")
    tp_place = lax.axis_index("tp")
    experts = expert_router.shape[1]
    block_len = expert_input.shape[0] // tp_count
    slots_each = 4 * block_len // experts

    def near(own):
        return [swapped(own, 1), swapped(own, 3)]

    gates = [gate_weight[0]] + near(gate_weight[0])
    ups = [up_weight[0]] + near(up_weight[0])
    gates.append(swapped(gates[2], 1))
    ups.append(swapped(ups[1], 3))
    downs, start = [], 0
    for width in WIDTHS:
        own = down_weight[0][:, start : start + width]
        start += width
        half = own.shape[0] // 2
        near_a, near_b = near(own)
        far_a = swapped(near_b[:half], 1)
        far_b = swapped(near_a[half:], 3)
        downs.append([own, near_a, near_b, far_a, far_b])

    own_input = lax.dynamic_slice_in_dim(expert_input, tp_place * block_len, block_len, 0)
    own_routes = lax.dynamic_slice_in_dim(routes, tp_place * block_len, block_len, 0)
    normed, pick, payload = dispatch(own_input, expert_gain, own_routes, experts, slots_each)
    rows = exchange(payload, experts)

    partial_rows = mixer_partial(mixer_input, mixer_gain, pool_in, pool_map, pool_scale, pool_out)
    mixer_output = mixer_reduce(partial_rows)
    weight = route_weights(normed, group_router, expert_router, own_routes)

    hidden = []
    for gate_w, up_w in zip(gates, ups):
        hidden.append(hidden_of(rows, [gate_w], [up_w]))
    expert_output = None
    for index, parts in enumerate(downs):
        most = down_of(hidden[:3], parts[:3], None, jnp.float32)
        result = down_of(hidden[3:], parts[3:], most, jnp.bfloat16)
        returned = exchange(result, experts)
        expert_output = combine(returned, pick, weight, index, expert_output)
    return (mixer_output, expert_output)


def solution(mesh):
    return jax.shard_map(
        layer,
        mesh=mesh,
        in_specs=(
            P("ep", None),
            P(),
            P(None, "tp"),
            P("tp", None, None),
            P("tp"),
            P("tp", None),
            P("ep", None),
            P(),
            P(),
            P(),
            P("ep", None),
            P("ep", None, "tp"),
            P("ep", None, "tp"),
            P("ep", "tp", None),
        ),
        out_specs=(P(("ep", "tp"), None), P(("ep", "tp"), None)),
        check_vma=False,
    )
```

```python
import jax
import jax.numpy as jnp
from jax import lax
from jax.experimental import pallas as pl
from jax.experimental.pallas import tpu as pltpu
from jax.sharding import PartitionSpec as P


RIM = 15
EPS = 1e-06
WIDTHS = (768, 1280)


def passed_along(value, axis, steps):
    count = lax.axis_size(axis)
    leading, last = (max(0, -steps), min(count, count - steps))
    return lax.ppermute(value, axis, [(source, source + steps) for source in range(leading, last)])


def swapped(value, mask):
    count = lax.axis_size("tp")
    return lax.ppermute(value, "tp", [(source, source ^ mask) for source in range(count)])


def norm_rows(values, gain):
    floats = values.astype(jnp.float32)
    scale = lax.rsqrt(jnp.mean(floats * floats, axis=-1, keepdims=True) + EPS)
    return (floats * scale * gain.astype(jnp.float32)).astype(jnp.bfloat16)


def mixer_partial(mixer_input, mixer_gain, pool_in, pool_map, pool_scale, pool_out):
    normed = norm_rows(mixer_input, mixer_gain)
    pooled_in = jnp.dot(normed, pool_in, preferred_element_type=jnp.float32).astype(jnp.bfloat16)
    local_rows = pooled_in.shape[0]
    groups_here = pool_map.shape[0]
    channels = pool_map.shape[1]
    border = passed_along(pooled_in[local_rows - RIM :], "ep", 1)
    padded = jnp.concatenate([border, pooled_in], axis=0).astype(jnp.float32)
    padded = padded.reshape(local_rows + RIM, groups_here, channels)
    leading = lax.axis_index("tp") * groups_here
    windows = jnp.left_shift(jnp.int32(2), leading + jnp.arange(groups_here, dtype=jnp.int32))
    window_sum = jnp.zeros((local_rows, groups_here, channels), jnp.float32)
    for offset in range(RIM + 1):
        active = (offset < windows).astype(jnp.float32)
        window_sum = (
            window_sum + padded[RIM - offset : RIM - offset + local_rows] * active[None, :, None]
        )
    position = lax.axis_index("ep") * local_rows + jnp.arange(local_rows, dtype=jnp.int32)
    counts_here = jnp.minimum(position[:, None] + 1, windows[None, :]).astype(jnp.float32)
    pooled = (window_sum / counts_here[:, :, None] - padded[RIM:]).astype(jnp.bfloat16)
    mapped = jnp.einsum("tgc,gce->tge", pooled, pool_map, preferred_element_type=jnp.float32)
    mixed_rows = (
        mapped.reshape(local_rows, groups_here * channels) * pool_scale.astype(jnp.float32)
    ).astype(jnp.bfloat16)
    return jnp.dot(mixed_rows, pool_out, preferred_element_type=jnp.float32).astype(jnp.bfloat16)


def mixer_reduce(partial_rows):
    count = lax.axis_size("tp")
    place = lax.axis_index("tp")
    rows = partial_rows.shape[0] // count

    def piece(k):
        return lax.dynamic_slice_in_dim(partial_rows, (place ^ k) * rows, rows, 0)

    total = piece(0).astype(jnp.float32)
    for k in range(1, count):
        part = piece(k)
        total = total + swapped(part, k).astype(jnp.float32)
    return total.astype(jnp.bfloat16)


def dispatch_kernel(x_ref, gain_ref, routes_ref, *outs):
    normed_ref, pick_ref, payload_ref = outs
    tokens = x_ref.shape[0]
    floats = x_ref[...].astype(jnp.float32)
    scale = lax.rsqrt(jnp.mean(floats * floats, axis=-1, keepdims=True) + EPS)
    normed = (floats * scale * gain_ref[...].astype(jnp.float32)).astype(jnp.bfloat16)
    normed_ref[...] = normed
    routes = routes_ref[...]
    slots = pick_ref.shape[2]
    experts = 64
    each = slots // experts
    expert = lax.broadcasted_iota(jnp.int32, (tokens, experts), 1)
    first = routes[:, 0:1] == expert
    second = routes[:, 1:2] == expert
    named = jnp.where(first | second, 1.0, 0.0)
    earlier = lax.broadcasted_iota(jnp.int32, (tokens, tokens), 1) < lax.broadcasted_iota(
        jnp.int32, (tokens, tokens), 0
    )
    before = jnp.dot(
        jnp.where(earlier, 1.0, 0.0).astype(jnp.bfloat16),
        named.astype(jnp.bfloat16),
        preferred_element_type=jnp.float32,
    )
    spread = lax.broadcasted_iota(jnp.int32, (experts, slots), 1) // each == lax.broadcasted_iota(
        jnp.int32, (experts, slots), 0
    )
    spread = jnp.where(spread, 1.0, 0.0).astype(jnp.bfloat16)
    within = (lax.broadcasted_iota(jnp.int32, (tokens, slots), 1) % each).astype(jnp.float32)
    chosen = []
    for mask in (first, second):
        place = jnp.where(mask, before, -1.0).astype(jnp.bfloat16)
        spread_place = jnp.dot(place, spread, preferred_element_type=jnp.float32)
        chosen.append(jnp.where(spread_place == within, 1.0, 0.0))
    pick_ref[0] = chosen[0].astype(jnp.bfloat16)
    pick_ref[1] = chosen[1].astype(jnp.bfloat16)
    either = (chosen[0] + chosen[1]).astype(jnp.bfloat16)
    payload = lax.dot_general(
        either, normed, (((0,), (0,)), ((), ())), preferred_element_type=jnp.float32
    )
    payload_ref[...] = payload.astype(jnp.bfloat16).reshape(payload_ref.shape)


def dispatch(x, gain, routes, experts, slots_each):
    tokens, model = x.shape
    slots = experts * slots_each
    return pl.pallas_call(
        dispatch_kernel,
        out_shape=[
            jax.ShapeDtypeStruct((tokens, model), jnp.bfloat16),
            jax.ShapeDtypeStruct((2, tokens, slots), jnp.bfloat16),
            jax.ShapeDtypeStruct((experts, slots_each // 2, 2, model), jnp.bfloat16),
        ],
        compiler_params=pltpu.CompilerParams(vmem_limit_bytes=16 << 20),
        name="dispatch",
    )(x, gain.reshape(1, model), routes)


def route_weights(rows, group_router, expert_router, route_rows):
    group_logits = jnp.dot(rows, group_router, preferred_element_type=jnp.float32)
    expert_logits = jnp.dot(rows, expert_router, preferred_element_type=jnp.float32)
    groups = group_logits.shape[1]
    experts = expert_logits.shape[1]
    member = (
        jnp.arange(experts, dtype=jnp.int32)[:, None] // (experts // groups)
        == jnp.arange(groups, dtype=jnp.int32)[None, :]
    ).astype(jnp.float32)
    group_exp = jnp.exp(group_logits)
    group_prob = group_exp / jnp.sum(group_exp, axis=1, keepdims=True)
    expert_exp = jnp.exp(expert_logits)
    within = jnp.dot(expert_exp, member, precision=lax.Precision.HIGHEST)
    prob = expert_exp * jnp.dot(group_prob / within, member.T, precision=lax.Precision.HIGHEST)
    chosen = (route_rows[:, :, None] == jnp.arange(experts, dtype=jnp.int32)[None, None, :]).astype(
        jnp.float32
    )
    picked = jnp.sum(chosen * prob[:, None, :], axis=2)
    return picked / jnp.sum(picked, axis=1, keepdims=True)


def combine_kernel(returned_ref, pick_ref, weight_ref, *refs):
    out_ref = refs[-1]
    width = returned_ref.shape[-1]
    returned = returned_ref[...].reshape(pick_ref.shape[2], width)
    weight = weight_ref[...]
    total = jnp.dot(pick_ref[0], returned, preferred_element_type=jnp.float32) * weight[:, 0:1]
    total = total + jnp.dot(pick_ref[1], returned, preferred_element_type=jnp.float32) * weight[:, 1:2]
    start = out_ref.shape[1] - width
    out_ref[:, start:] = total.astype(jnp.bfloat16)
    if start:
        out_ref[:, :start] = refs[0][...]


def combine(returned, pick, weight, so_far):
    before = [] if so_far is None else [so_far]
    width = returned.shape[-1] + sum(part.shape[1] for part in before)
    return pl.pallas_call(
        combine_kernel,
        out_shape=jax.ShapeDtypeStruct((pick.shape[1], width), jnp.bfloat16),
        compiler_params=pltpu.CompilerParams(vmem_limit_bytes=8 << 20),
        name="combine",
    )(returned, pick, weight, *before)


def hidden_kernel(rows_ref, gate_ref, up_ref, out_ref, *flat_ref):
    rows = rows_ref[...]
    if flat_ref:
        rows = rows.reshape(flat_ref[0].shape)
        flat_ref[0][...] = rows
    gate = jnp.dot(rows, gate_ref[...], preferred_element_type=jnp.float32)
    up = jnp.dot(rows, up_ref[...], preferred_element_type=jnp.float32)
    out_ref[...] = (gate / (1.0 + jnp.exp(-gate)) * up).astype(jnp.bfloat16)


def hidden_of(rows, gate_part, up_part):
    model, units = gate_part.shape
    count = rows.size // model
    shapes = [jax.ShapeDtypeStruct((count, units), jnp.bfloat16)]
    if rows.ndim > 2:
        shapes.append(jax.ShapeDtypeStruct((count, model), jnp.bfloat16))
    return pl.pallas_call(
        hidden_kernel,
        out_shape=shapes,
        compiler_params=pltpu.CompilerParams(vmem_limit_bytes=12 << 20),
        cost_estimate=pl.CostEstimate(
            flops=4 * count * model * units, bytes_accessed=4 << 20, transcendentals=0
        ),
        name="hidden",
    )(rows, gate_part, up_part)


def down_kernel(hidden_refs, down_refs, base_ref, out_ref):
    total = None if base_ref is None else base_ref[...]
    index, start = 0, 0
    for part in down_refs:
        depth = part.shape[0]
        piece = jnp.dot(
            hidden_refs[index][:, start : start + depth],
            part[...],
            preferred_element_type=jnp.float32,
        )
        total = piece if total is None else total + piece
        start += depth
        if start == hidden_refs[index].shape[1]:
            index, start = index + 1, 0
    out_ref[...] = total.astype(out_ref.dtype).reshape(out_ref.shape)


def down_of(hidden, parts, base, out_shape):
    rows, width = hidden[0].shape[0], parts[0].shape[1]
    depth = sum(part.shape[0] for part in parts)
    bases = [] if base is None else [base]

    def kernel(*refs):
        refs = list(refs)
        hidden_refs, rest = refs[: len(hidden)], refs[len(hidden) :]
        down_refs, rest = rest[: len(parts)], rest[len(parts) :]
        down_kernel(hidden_refs, down_refs, rest[0] if bases else None, rest[-1])

    return pl.pallas_call(
        kernel,
        out_shape=out_shape,
        compiler_params=pltpu.CompilerParams(vmem_limit_bytes=12 << 20),
        cost_estimate=pl.CostEstimate(
            flops=2 * rows * depth * width, bytes_accessed=4 << 20, transcendentals=0
        ),
        name="down",
    )(*hidden, *parts, *bases)


def exchange(rows):
    return lax.all_to_all(rows, "ep", split_axis=0, concat_axis=0, tiled=True)


def layer(
    mixer_input,
    mixer_gain,
    pool_in,
    pool_map,
    pool_scale,
    pool_out,
    expert_input,
    expert_gain,
    group_router,
    expert_router,
    routes,
    gate_weight,
    up_weight,
    down_weight,
):
    tp_count = lax.axis_size("tp")
    tp_place = lax.axis_index("tp")
    experts = expert_router.shape[1]
    block_len = expert_input.shape[0] // tp_count
    slots_each = 4 * block_len // experts

    def near(own):
        return [swapped(own, 1), swapped(own, 3)]

    gates = [gate_weight[0]] + near(gate_weight[0])
    ups = [up_weight[0]] + near(up_weight[0])
    gates.append(swapped(gates[2], 1))
    ups.append(swapped(ups[1], 3))
    downs, start = [], 0
    for width in WIDTHS:
        half = down_weight.shape[1] // 2
        own = [down_weight[0, i * half : (i + 1) * half, start : start + width] for i in range(2)]
        start += width
        lows = near(own[0])
        highs = near(own[1])
        far_low = swapped(lows[1], 1)
        far_high = swapped(highs[0], 3)
        downs.append(own + [lows[0], highs[0], lows[1], highs[1], far_low, far_high])

    own_input = lax.dynamic_slice_in_dim(expert_input, tp_place * block_len, block_len, 0)
    own_routes = lax.dynamic_slice_in_dim(routes, tp_place * block_len, block_len, 0)
    normed, pick, payload = dispatch(own_input, expert_gain, own_routes, experts, slots_each)
    rows = exchange(payload)

    partial_rows = mixer_partial(mixer_input, mixer_gain, pool_in, pool_map, pool_scale, pool_out)
    mixer_output = mixer_reduce(partial_rows)
    weight = route_weights(normed, group_router, expert_router, own_routes)

    hidden = []
    for gate_w, up_w in zip(gates, ups):
        part, *flat = hidden_of(rows, gate_w, up_w)
        hidden.append(part)
        rows = flat[0] if flat else rows
    expert_output = None
    for index, parts in enumerate(downs):
        most = down_of(
            hidden[:3],
            parts[:-2],
            None,
            jax.ShapeDtypeStruct((rows.shape[0], WIDTHS[index]), jnp.float32),
        )
        result = down_of(
            hidden[3:],
            parts[-2:],
            most,
            jax.ShapeDtypeStruct(payload.shape[:3] + (WIDTHS[index],), jnp.bfloat16),
        )
        returned = exchange(result)
        expert_output = combine(returned, pick, weight, expert_output)
    return (mixer_output, expert_output)


def solution(mesh):
    return jax.shard_map(
        layer,
        mesh=mesh,
        in_specs=(
            P("ep", None),
            P(),
            P(None, "tp"),
            P("tp", None, None),
            P("tp"),
            P("tp", None),
            P("ep", None),
            P(),
            P(),
            P(),
            P("ep", None),
            P("ep", None, "tp"),
            P("ep", None, "tp"),
            P("ep", "tp", None),
        ),
        out_specs=(P(("ep", "tp"), None), P(("ep", "tp"), None)),
        check_vma=False,
    )
```

```python
import jax
import jax.numpy as jnp
from jax import lax
from jax.experimental import pallas as pl
from jax.experimental.pallas import tpu as pltpu
from jax.sharding import PartitionSpec as P


RIM = 15
EPS = 1e-06


def passed_along(value, axis, steps):
    count = lax.axis_size(axis)
    leading, last = (max(0, -steps), min(count, count - steps))
    return lax.ppermute(value, axis, [(source, source + steps) for source in range(leading, last)])


def swapped(value, mask):
    count = lax.axis_size("tp")
    return lax.ppermute(value, "tp", [(source, source ^ mask) for source in range(count)])


def sent(value, holder_moves, other_moves):
    count = lax.axis_size("tp")
    pairs = []
    for device in range(lax.axis_size("ep")):
        for place in range(count):
            mask, to_holder = holder_moves if device % 2 == place % 2 else other_moves
            goal = place ^ mask
            core = goal % 2 if to_holder else 1 - goal % 2
            pairs.append((device * count + place, (device - device % 2 + core) * count + goal))
    return lax.ppermute(value, ("ep", "tp"), pairs)


def parts_of(own):
    first = sent(own, (0, False), (1, True))
    second = sent(own, (2, False), (3, True))
    first_over = sent(first, (0, False), (0, True))
    second_over = sent(second, (0, False), (0, True))
    return [(own, first), (first, first_over), (second, second_over), (second_over, second)]


def norm_rows(values, gain):
    floats = values.astype(jnp.float32)
    scale = lax.rsqrt(jnp.mean(floats * floats, axis=-1, keepdims=True) + EPS)
    return (floats * scale * gain.astype(jnp.float32)).astype(jnp.bfloat16)


def mixer_partial(mixer_input, mixer_gain, pool_in, pool_map, pool_scale, pool_out):
    normed = norm_rows(mixer_input, mixer_gain)
    pooled_in = jnp.dot(normed, pool_in, preferred_element_type=jnp.float32).astype(jnp.bfloat16)
    local_rows = pooled_in.shape[0]
    groups_here = pool_map.shape[0]
    channels = pool_map.shape[1]
    last = norm_rows(mixer_input[local_rows - RIM - 1 :], mixer_gain)
    last = jnp.dot(last, pool_in, preferred_element_type=jnp.float32).astype(jnp.bfloat16)
    border = passed_along(last[1:], "ep", 1)
    padded = jnp.concatenate([border, pooled_in], axis=0).astype(jnp.float32)
    padded = padded.reshape(local_rows + RIM, groups_here, channels)
    leading = lax.axis_index("tp") * groups_here
    windows = jnp.left_shift(jnp.int32(2), leading + jnp.arange(groups_here, dtype=jnp.int32))
    window_sum = jnp.zeros((local_rows, groups_here, channels), jnp.float32)
    for offset in range(RIM + 1):
        active = (offset < windows).astype(jnp.float32)
        window_sum = (
            window_sum + padded[RIM - offset : RIM - offset + local_rows] * active[None, :, None]
        )
    position = lax.axis_index("ep") * local_rows + jnp.arange(local_rows, dtype=jnp.int32)
    counts_here = jnp.minimum(position[:, None] + 1, windows[None, :]).astype(jnp.float32)
    pooled = (window_sum / counts_here[:, :, None] - padded[RIM:]).astype(jnp.bfloat16)
    mapped = jnp.einsum("tgc,gce->tge", pooled, pool_map, preferred_element_type=jnp.float32)
    mixed_rows = (
        mapped.reshape(local_rows, groups_here * channels) * pool_scale.astype(jnp.float32)
    ).astype(jnp.bfloat16)
    return jnp.dot(mixed_rows, pool_out, preferred_element_type=jnp.float32).astype(jnp.bfloat16)


def mixer_reduce(partial_rows):
    count = lax.axis_size("tp")
    place = lax.axis_index("tp")
    rows = partial_rows.shape[0] // count

    def piece(k):
        return lax.dynamic_slice_in_dim(partial_rows, (place ^ k) * rows, rows, 0)

    total = piece(0).astype(jnp.float32)
    for k in range(1, count):
        part = piece(k)
        total = total + swapped(part, k).astype(jnp.float32)
    return total.astype(jnp.bfloat16)


def dispatch_kernel(x_ref, gain_ref, targets_ref, *outs):
    normed_ref, pick_ref, payload_ref = outs
    tokens = x_ref.shape[0]
    floats = x_ref[...].astype(jnp.float32)
    scale = lax.rsqrt(jnp.mean(floats * floats, axis=-1, keepdims=True) + EPS)
    normed = (floats * scale * gain_ref[...].astype(jnp.float32)).astype(jnp.bfloat16)
    normed_ref[...] = normed
    targets = targets_ref[...]
    slots = pick_ref.shape[2]
    experts = 64
    each = slots // experts
    expert = lax.broadcasted_iota(jnp.int32, (tokens, experts), 1)
    first = targets[:, 0:1] == expert
    second = targets[:, 1:2] == expert
    named = jnp.where(first | second, 1.0, 0.0)
    earlier = lax.broadcasted_iota(jnp.int32, (tokens, tokens), 1) < lax.broadcasted_iota(
        jnp.int32, (tokens, tokens), 0
    )
    before = jnp.dot(
        jnp.where(earlier, 1.0, 0.0).astype(jnp.bfloat16),
        named.astype(jnp.bfloat16),
        preferred_element_type=jnp.float32,
    )
    spread = lax.broadcasted_iota(jnp.int32, (experts, slots), 1) // each == lax.broadcasted_iota(
        jnp.int32, (experts, slots), 0
    )
    spread = jnp.where(spread, 1.0, 0.0).astype(jnp.bfloat16)
    within = (lax.broadcasted_iota(jnp.int32, (tokens, slots), 1) % each).astype(jnp.float32)
    chosen = []
    for mask in (first, second):
        place = jnp.where(mask, before, -1.0).astype(jnp.bfloat16)
        spread_place = jnp.dot(place, spread, preferred_element_type=jnp.float32)
        chosen.append(jnp.where(spread_place == within, 1.0, 0.0))
    pick_ref[0] = chosen[0].astype(jnp.bfloat16)
    pick_ref[1] = chosen[1].astype(jnp.bfloat16)
    either = (chosen[0] + chosen[1]).astype(jnp.bfloat16)
    payload = lax.dot_general(
        either, normed, (((0,), (0,)), ((), ())), preferred_element_type=jnp.float32
    )
    payload_ref[...] = payload.astype(jnp.bfloat16).reshape(payload_ref.shape)


def dispatch(x, gain, targets, experts, slots_each):
    tokens, model = x.shape
    slots = experts * slots_each
    return pl.pallas_call(
        dispatch_kernel,
        out_shape=[
            jax.ShapeDtypeStruct((tokens, model), jnp.bfloat16),
            jax.ShapeDtypeStruct((2, tokens, slots), jnp.bfloat16),
            jax.ShapeDtypeStruct((experts, slots_each // 2, 2, model), jnp.bfloat16),
        ],
        compiler_params=pltpu.CompilerParams(vmem_limit_bytes=16 << 20),
        name="dispatch",
    )(x, gain.reshape(1, model), targets)


def route_weights(rows, group_router, expert_router, route_rows):
    group_logits = jnp.dot(rows, group_router, preferred_element_type=jnp.float32)
    expert_logits = jnp.dot(rows, expert_router, preferred_element_type=jnp.float32)
    groups = group_logits.shape[1]
    experts = expert_logits.shape[1]
    member = (
        jnp.arange(experts, dtype=jnp.int32)[:, None] // (experts // groups)
        == jnp.arange(groups, dtype=jnp.int32)[None, :]
    ).astype(jnp.float32)
    group_exp = jnp.exp(group_logits)
    group_prob = group_exp / jnp.sum(group_exp, axis=1, keepdims=True)
    expert_exp = jnp.exp(expert_logits)
    within = jnp.dot(expert_exp, member, precision=lax.Precision.HIGHEST)
    prob = expert_exp * jnp.dot(group_prob / within, member.T, precision=lax.Precision.HIGHEST)
    chosen = (route_rows[:, :, None] == jnp.arange(experts, dtype=jnp.int32)[None, None, :]).astype(
        jnp.float32
    )
    picked = jnp.sum(chosen * prob[:, None, :], axis=2)
    return picked / jnp.sum(picked, axis=1, keepdims=True)


def combine_kernel(returned_ref, pick_ref, weight_ref, own_ref, other_ref):
    returned = returned_ref[...].reshape(pick_ref.shape[2], returned_ref.shape[-1])
    weight = weight_ref[...]
    total = jnp.dot(pick_ref[0], returned, preferred_element_type=jnp.float32) * weight[:, 0:1]
    total = total + jnp.dot(pick_ref[1], returned, preferred_element_type=jnp.float32) * weight[:, 1:2]
    rows = own_ref.shape[0]
    own_ref[...] = total[:rows]
    other_ref[...] = total[rows:].astype(jnp.bfloat16)


def combine(returned, pick, weight):
    shape = (pick.shape[1] // 2, returned.shape[-1])
    return pl.pallas_call(
        combine_kernel,
        out_shape=[
            jax.ShapeDtypeStruct(shape, jnp.float32),
            jax.ShapeDtypeStruct(shape, jnp.bfloat16),
        ],
        compiler_params=pltpu.CompilerParams(vmem_limit_bytes=12 << 20),
        name="combine",
    )(returned, pick, weight)


def fetch(flag_ref, pair, target, sem):
    @pl.when(flag_ref[0] == 1)
    def _():
        pltpu.make_async_copy(pair[0], target, sem).start()

    @pl.when(flag_ref[0] != 1)
    def _():
        pltpu.make_async_copy(pair[1], target, sem).start()

    return pltpu.make_async_copy(pair[0], target, sem)


def hidden_kernel(flag_ref, rows_ref, *refs):
    out_ref, gate_scratch, up_scratch, sems = refs[-4:]
    count = gate_scratch.shape[0]
    units = gate_scratch.shape[2]

    def start(q):
        pairs = (refs[4 * q], refs[4 * q + 1]), (refs[4 * q + 2], refs[4 * q + 3])
        targets = gate_scratch.at[q], up_scratch.at[q]
        return [fetch(flag_ref, pairs[i], targets[i], sems.at[q, i]) for i in range(2)]

    waits = [start(0), start(1)]
    rows = rows_ref[...].reshape(out_ref.shape[0], rows_ref.shape[-1])
    for q in range(count):
        waits[q][0].wait()
        waits[q][1].wait()
        if q + 2 < count:
            waits.append(start(q + 2))
        gate = jnp.dot(rows, gate_scratch[q], preferred_element_type=jnp.float32)
        up = jnp.dot(rows, up_scratch[q], preferred_element_type=jnp.float32)
        out_ref[:, q * units : (q + 1) * units] = (gate / (1.0 + jnp.exp(-gate)) * up).astype(
            jnp.bfloat16
        )


def hidden_of(flag, rows, gates, ups):
    model, units = gates[0][0].shape
    count = rows.size // model
    parts = len(gates)
    arrays = [array for gate, up in zip(gates, ups) for array in (*gate, *up)]
    return pl.pallas_call(
        hidden_kernel,
        out_shape=jax.ShapeDtypeStruct((count, parts * units), jnp.bfloat16),
        in_specs=[
            pl.BlockSpec(memory_space=pltpu.SMEM),
            pl.BlockSpec(memory_space=pltpu.VMEM),
        ]
        + [pl.BlockSpec(memory_space=pltpu.HBM)] * len(arrays),
        scratch_shapes=[
            pltpu.VMEM((parts, model, units), jnp.bfloat16),
            pltpu.VMEM((parts, model, units), jnp.bfloat16),
            pltpu.SemaphoreType.DMA((parts, 2)),
        ],
        compiler_params=pltpu.CompilerParams(vmem_limit_bytes=58 << 20),
        cost_estimate=pl.CostEstimate(
            flops=4 * count * model * units * parts, bytes_accessed=9 << 20, transcendentals=0
        ),
        name="hidden",
    )(flag, rows, *arrays)


DOWN_COLUMNS = 512


def down_kernel(flag_ref, hidden_ref, *refs):
    out_ref, scratch, result, sems, out_sems = refs[-5:]
    parts, units, model = scratch.shape
    steps = model // DOWN_COLUMNS
    waits = []
    for n in range(steps):
        columns = pl.ds(n * DOWN_COLUMNS, DOWN_COLUMNS)
        waits.append(
            [
                fetch(
                    flag_ref,
                    (refs[2 * q].at[:, columns], refs[2 * q + 1].at[:, columns]),
                    scratch.at[q, :, columns],
                    sems.at[n, q],
                )
                for q in range(parts)
            ]
        )
    leaving = []
    for n in range(steps):
        columns = slice(n * DOWN_COLUMNS, (n + 1) * DOWN_COLUMNS)
        total = None
        for q in range(parts):
            waits[n][q].wait()
            piece = jnp.dot(
                hidden_ref[:, q * units : (q + 1) * units],
                scratch[q, :, columns],
                preferred_element_type=jnp.float32,
            )
            total = piece if total is None else total + piece
        result[n] = total.astype(jnp.bfloat16).reshape(result.shape[1:])
        leaving.append(
            pltpu.make_async_copy(
                result.at[n],
                out_ref.at[:, :, :, pl.ds(n * DOWN_COLUMNS, DOWN_COLUMNS)],
                out_sems.at[n],
            )
        )
        leaving[-1].start()
    for copy in leaving:
        copy.wait()


def down_of(flag, hidden, downs, out_shape):
    units, model = downs[0][0].shape
    parts = len(downs)
    arrays = [array for pair in downs for array in pair]
    return pl.pallas_call(
        down_kernel,
        out_shape=out_shape,
        in_specs=[
            pl.BlockSpec(memory_space=pltpu.SMEM),
            pl.BlockSpec(memory_space=pltpu.VMEM),
        ]
        + [pl.BlockSpec(memory_space=pltpu.HBM)] * len(arrays),
        out_specs=pl.BlockSpec(memory_space=pltpu.HBM),
        scratch_shapes=[
            pltpu.VMEM((parts, units, model), jnp.bfloat16),
            pltpu.VMEM(
                (model // DOWN_COLUMNS,) + out_shape.shape[:3] + (DOWN_COLUMNS,), jnp.bfloat16
            ),
            pltpu.SemaphoreType.DMA((model // DOWN_COLUMNS, parts)),
            pltpu.SemaphoreType.DMA((model // DOWN_COLUMNS,)),
        ],
        compiler_params=pltpu.CompilerParams(vmem_limit_bytes=58 << 20),
        cost_estimate=pl.CostEstimate(
            flops=2 * hidden.size * model, bytes_accessed=6 << 20, transcendentals=0
        ),
        name="down",
    )(flag, hidden, *arrays)


def exchange(rows):
    return lax.all_to_all(rows, "ep", split_axis=0, concat_axis=0, tiled=True)


def layer(
    mixer_input,
    mixer_gain,
    pool_in,
    pool_map,
    pool_scale,
    pool_out,
    expert_input,
    expert_gain,
    group_router,
    expert_router,
    routes,
    gate_weight,
    up_weight,
    down_weight,
):
    tp_count = lax.axis_size("tp")
    tp_place = lax.axis_index("tp")
    experts = expert_router.shape[1]
    block_len = expert_input.shape[0] // tp_count
    slots_each = 4 * block_len // experts

    gates = parts_of(gate_weight[0])
    ups = parts_of(up_weight[0])
    downs = parts_of(down_weight[0])

    starts = [tp_place * block_len, (tp_place ^ 1) * block_len]
    pair_input = jnp.concatenate(
        [lax.dynamic_slice_in_dim(expert_input, start, block_len, 0) for start in starts], axis=0
    )
    pair_routes = jnp.concatenate(
        [lax.dynamic_slice_in_dim(routes, start, block_len, 0) for start in starts], axis=0
    )
    parity = tp_place % 2
    core = jnp.where(jnp.arange(2 * block_len) < block_len, parity, 1 - parity)[:, None]
    targets = jnp.where(pair_routes % 2 == parity, pair_routes - parity + core, -1)
    normed, pick, payload = dispatch(pair_input, expert_gain, targets, experts, slots_each)
    rows = exchange(payload)

    partial_rows = mixer_partial(mixer_input, mixer_gain, pool_in, pool_map, pool_scale, pool_out)
    mixer_output = mixer_reduce(partial_rows)
    weight = route_weights(normed, group_router, expert_router, pair_routes)

    flag = (lax.axis_index("ep") % 2 == parity).astype(jnp.int32).reshape(1)
    hidden = hidden_of(flag, rows, gates, ups)
    result = down_of(
        flag, hidden, downs, jax.ShapeDtypeStruct(payload.shape, jnp.bfloat16)
    )
    returned = exchange(result)
    own, other = combine(returned, pick, weight)
    expert_output = (own + swapped(other, 1).astype(jnp.float32)).astype(jnp.bfloat16)
    return (mixer_output, expert_output)


def solution(mesh):
    return jax.shard_map(
        layer,
        mesh=mesh,
        in_specs=(
            P("ep", None),
            P(),
            P(None, "tp"),
            P("tp", None, None),
            P("tp"),
            P("tp", None),
            P("ep", None),
            P(),
            P(),
            P(),
            P("ep", None),
            P("ep", None, "tp"),
            P("ep", None, "tp"),
            P("ep", "tp", None),
        ),
        out_specs=(P(("ep", "tp"), None), P(("ep", "tp"), None)),
        check_vma=False,
    )
```

```python
import jax
import jax.numpy as jnp
from jax import lax
from jax.experimental import pallas as pl
from jax.experimental.pallas import tpu as pltpu
from jax.sharding import PartitionSpec as P


RIM = 15
EPS = 1e-06


def passed_along(value, axis, steps):
    count = lax.axis_size(axis)
    leading, last = (max(0, -steps), min(count, count - steps))
    return lax.ppermute(value, axis, [(source, source + steps) for source in range(leading, last)])


def swapped(value, mask):
    count = lax.axis_size("tp")
    return lax.ppermute(value, "tp", [(source, source ^ mask) for source in range(count)])


def sent(value, holder_moves, other_moves):
    count = lax.axis_size("tp")
    pairs = []
    for device in range(lax.axis_size("ep")):
        for place in range(count):
            mask, to_holder = holder_moves if device % 2 == place % 2 else other_moves
            goal = place ^ mask
            core = goal % 2 if to_holder else 1 - goal % 2
            pairs.append((device * count + place, (device - device % 2 + core) * count + goal))
    return lax.ppermute(value, ("ep", "tp"), pairs)


def parts_of(own):
    first = sent(own, (0, False), (1, True))
    second = sent(own, (2, False), (3, True))
    first_over = sent(first, (0, False), (0, True))
    second_over = sent(second, (0, False), (0, True))
    return [(own, first), (first, first_over), (second, second_over), (second_over, second)]


def norm_rows(values, gain):
    floats = values.astype(jnp.float32)
    scale = lax.rsqrt(jnp.mean(floats * floats, axis=-1, keepdims=True) + EPS)
    return (floats * scale * gain.astype(jnp.float32)).astype(jnp.bfloat16)


def mixer_partial(mixer_input, mixer_gain, pool_in, pool_map, pool_scale, pool_out):
    normed = norm_rows(mixer_input, mixer_gain)
    pooled_in = jnp.dot(normed, pool_in, preferred_element_type=jnp.float32).astype(jnp.bfloat16)
    local_rows = pooled_in.shape[0]
    groups_here = pool_map.shape[0]
    channels = pool_map.shape[1]
    last = norm_rows(mixer_input[local_rows - RIM - 1 :], mixer_gain)
    last = jnp.dot(last, pool_in, preferred_element_type=jnp.float32).astype(jnp.bfloat16)
    border = passed_along(last[1:], "ep", 1)
    padded = jnp.concatenate([border, pooled_in], axis=0).astype(jnp.float32)
    padded = padded.reshape(local_rows + RIM, groups_here, channels)
    leading = lax.axis_index("tp") * groups_here
    windows = jnp.left_shift(jnp.int32(2), leading + jnp.arange(groups_here, dtype=jnp.int32))
    window_sum = jnp.zeros((local_rows, groups_here, channels), jnp.float32)
    for offset in range(RIM + 1):
        active = (offset < windows).astype(jnp.float32)
        window_sum = (
            window_sum + padded[RIM - offset : RIM - offset + local_rows] * active[None, :, None]
        )
    position = lax.axis_index("ep") * local_rows + jnp.arange(local_rows, dtype=jnp.int32)
    counts_here = jnp.minimum(position[:, None] + 1, windows[None, :]).astype(jnp.float32)
    pooled = (window_sum / counts_here[:, :, None] - padded[RIM:]).astype(jnp.bfloat16)
    mapped = jnp.einsum("tgc,gce->tge", pooled, pool_map, preferred_element_type=jnp.float32)
    mixed_rows = (
        mapped.reshape(local_rows, groups_here * channels) * pool_scale.astype(jnp.float32)
    ).astype(jnp.bfloat16)
    return jnp.dot(mixed_rows, pool_out, preferred_element_type=jnp.float32).astype(jnp.bfloat16)


def mixer_reduce(partial_rows):
    count = lax.axis_size("tp")
    place = lax.axis_index("tp")
    rows = partial_rows.shape[0] // count

    def piece(k):
        return lax.dynamic_slice_in_dim(partial_rows, (place ^ k) * rows, rows, 0)

    total = piece(0).astype(jnp.float32)
    for k in range(1, count):
        part = piece(k)
        total = total + swapped(part, k).astype(jnp.float32)
    return total.astype(jnp.bfloat16)


def dispatch_kernel(x_ref, gain_ref, targets_ref, *outs):
    normed_ref, pick_ref, payload_ref = outs
    tokens = x_ref.shape[0]
    floats = x_ref[...].astype(jnp.float32)
    scale = lax.rsqrt(jnp.mean(floats * floats, axis=-1, keepdims=True) + EPS)
    normed = (floats * scale * gain_ref[...].astype(jnp.float32)).astype(jnp.bfloat16)
    normed_ref[...] = normed
    targets = targets_ref[...]
    slots = pick_ref.shape[2]
    experts = 64
    each = slots // experts
    expert = lax.broadcasted_iota(jnp.int32, (tokens, experts), 1)
    first = targets[:, 0:1] == expert
    second = targets[:, 1:2] == expert
    named = jnp.where(first | second, 1.0, 0.0)
    earlier = lax.broadcasted_iota(jnp.int32, (tokens, tokens), 1) < lax.broadcasted_iota(
        jnp.int32, (tokens, tokens), 0
    )
    before = jnp.dot(
        jnp.where(earlier, 1.0, 0.0).astype(jnp.bfloat16),
        named.astype(jnp.bfloat16),
        preferred_element_type=jnp.float32,
    )
    spread = lax.broadcasted_iota(jnp.int32, (experts, slots), 1) // each == lax.broadcasted_iota(
        jnp.int32, (experts, slots), 0
    )
    spread = jnp.where(spread, 1.0, 0.0).astype(jnp.bfloat16)
    within = (lax.broadcasted_iota(jnp.int32, (tokens, slots), 1) % each).astype(jnp.float32)
    chosen = []
    for mask in (first, second):
        place = jnp.where(mask, before, -1.0).astype(jnp.bfloat16)
        spread_place = jnp.dot(place, spread, preferred_element_type=jnp.float32)
        chosen.append(jnp.where(spread_place == within, 1.0, 0.0))
    pick_ref[0] = chosen[0].astype(jnp.bfloat16)
    pick_ref[1] = chosen[1].astype(jnp.bfloat16)
    either = (chosen[0] + chosen[1]).astype(jnp.bfloat16)
    payload = lax.dot_general(
        either, normed, (((0,), (0,)), ((), ())), preferred_element_type=jnp.float32
    )
    payload_ref[...] = payload.astype(jnp.bfloat16).reshape(payload_ref.shape)


def dispatch(x, gain, targets, experts, slots_each):
    tokens, model = x.shape
    slots = experts * slots_each
    return pl.pallas_call(
        dispatch_kernel,
        out_shape=[
            jax.ShapeDtypeStruct((tokens, model), jnp.bfloat16),
            jax.ShapeDtypeStruct((2, tokens, slots), jnp.bfloat16),
            jax.ShapeDtypeStruct((experts, slots_each // 2, 2, model), jnp.bfloat16),
        ],
        compiler_params=pltpu.CompilerParams(vmem_limit_bytes=16 << 20),
        name="dispatch",
    )(x, gain.reshape(1, model), targets)


def route_weights(rows, group_router, expert_router, route_rows):
    group_logits = jnp.dot(rows, group_router, preferred_element_type=jnp.float32)
    expert_logits = jnp.dot(rows, expert_router, preferred_element_type=jnp.float32)
    groups = group_logits.shape[1]
    experts = expert_logits.shape[1]
    member = (
        jnp.arange(experts, dtype=jnp.int32)[:, None] // (experts // groups)
        == jnp.arange(groups, dtype=jnp.int32)[None, :]
    ).astype(jnp.float32)
    group_exp = jnp.exp(group_logits)
    group_prob = group_exp / jnp.sum(group_exp, axis=1, keepdims=True)
    expert_exp = jnp.exp(expert_logits)
    within = jnp.dot(expert_exp, member, precision=lax.Precision.HIGHEST)
    prob = expert_exp * jnp.dot(group_prob / within, member.T, precision=lax.Precision.HIGHEST)
    chosen = (route_rows[:, :, None] == jnp.arange(experts, dtype=jnp.int32)[None, None, :]).astype(
        jnp.float32
    )
    picked = jnp.sum(chosen * prob[:, None, :], axis=2)
    return picked / jnp.sum(picked, axis=1, keepdims=True)


def combine_kernel(returned_ref, pick_ref, weight_ref, own_ref, other_ref):
    returned = returned_ref[...].reshape(pick_ref.shape[2], returned_ref.shape[-1])
    weight = weight_ref[...]
    total = jnp.dot(pick_ref[0], returned, preferred_element_type=jnp.float32) * weight[:, 0:1]
    total = total + jnp.dot(pick_ref[1], returned, preferred_element_type=jnp.float32) * weight[:, 1:2]
    rows = own_ref.shape[0]
    own_ref[...] = total[:rows]
    other_ref[...] = total[rows:].astype(jnp.bfloat16)


def combine(returned, pick, weight):
    shape = (pick.shape[1] // 2, returned.shape[-1])
    return pl.pallas_call(
        combine_kernel,
        out_shape=[
            jax.ShapeDtypeStruct(shape, jnp.float32),
            jax.ShapeDtypeStruct(shape, jnp.bfloat16),
        ],
        compiler_params=pltpu.CompilerParams(vmem_limit_bytes=12 << 20),
        name="combine",
    )(returned, pick, weight)


def fetch(flag_ref, pair, target, sem):
    @pl.when(flag_ref[0] == 1)
    def _():
        pltpu.make_async_copy(pair[0], target, sem).start()

    @pl.when(flag_ref[0] != 1)
    def _():
        pltpu.make_async_copy(pair[1], target, sem).start()

    return pltpu.make_async_copy(pair[0], target, sem)


def hidden_kernel(flag_ref, rows_ref, *refs):
    out_ref, gate_scratch, up_scratch, sems = refs[-4:]
    count = gate_scratch.shape[0]
    units = gate_scratch.shape[2]

    def start(q):
        pairs = (refs[4 * q], refs[4 * q + 1]), (refs[4 * q + 2], refs[4 * q + 3])
        targets = gate_scratch.at[q], up_scratch.at[q]
        return [fetch(flag_ref, pairs[i], targets[i], sems.at[q, i]) for i in range(2)]

    waits = [start(0), start(1)]
    rows = rows_ref[...].reshape(out_ref.shape[0], rows_ref.shape[-1])
    for q in range(count):
        waits[q][0].wait()
        waits[q][1].wait()
        if q + 2 < count:
            waits.append(start(q + 2))
        gate = jnp.dot(rows, gate_scratch[q], preferred_element_type=jnp.float32)
        up = jnp.dot(rows, up_scratch[q], preferred_element_type=jnp.float32)
        out_ref[:, q * units : (q + 1) * units] = (gate / (1.0 + jnp.exp(-gate)) * up).astype(
            jnp.bfloat16
        )


def hidden_of(flag, rows, gates, ups):
    model, units = gates[0][0].shape
    count = rows.size // model
    parts = len(gates)
    arrays = [array for gate, up in zip(gates, ups) for array in (*gate, *up)]
    return pl.pallas_call(
        hidden_kernel,
        out_shape=jax.ShapeDtypeStruct((count, parts * units), jnp.bfloat16),
        in_specs=[
            pl.BlockSpec(memory_space=pltpu.SMEM),
            pl.BlockSpec(memory_space=pltpu.VMEM),
        ]
        + [pl.BlockSpec(memory_space=pltpu.HBM)] * len(arrays),
        scratch_shapes=[
            pltpu.VMEM((parts, model, units), jnp.bfloat16),
            pltpu.VMEM((parts, model, units), jnp.bfloat16),
            pltpu.SemaphoreType.DMA((parts, 2)),
        ],
        compiler_params=pltpu.CompilerParams(vmem_limit_bytes=58 << 20),
        cost_estimate=pl.CostEstimate(
            flops=4 * count * model * units * parts, bytes_accessed=9 << 20, transcendentals=0
        ),
        name="hidden",
    )(flag, rows, *arrays)


DOWN_COLUMNS = 512


def down_kernel(flag_ref, hidden_ref, *refs):
    out_ref, scratch, sems = refs[-3:]
    parts, units, model = scratch.shape
    steps = model // DOWN_COLUMNS
    waits = []
    for n in range(steps):
        columns = pl.ds(n * DOWN_COLUMNS, DOWN_COLUMNS)
        waits.append(
            [
                fetch(
                    flag_ref,
                    (refs[2 * q].at[:, columns], refs[2 * q + 1].at[:, columns]),
                    scratch.at[q, :, columns],
                    sems.at[n, q],
                )
                for q in range(parts)
            ]
        )
    for n in range(steps):
        columns = slice(n * DOWN_COLUMNS, (n + 1) * DOWN_COLUMNS)
        total = None
        for q in range(parts):
            waits[n][q].wait()
            piece = jnp.dot(
                hidden_ref[:, q * units : (q + 1) * units],
                scratch[q, :, columns],
                preferred_element_type=jnp.float32,
            )
            total = piece if total is None else total + piece
        out_ref[:, :, :, columns] = total.astype(jnp.bfloat16).reshape(
            out_ref.shape[:3] + (DOWN_COLUMNS,)
        )


def down_of(flag, hidden, downs, out_shape):
    units, model = downs[0][0].shape
    parts = len(downs)
    arrays = [array for pair in downs for array in pair]
    return pl.pallas_call(
        down_kernel,
        out_shape=out_shape,
        in_specs=[
            pl.BlockSpec(memory_space=pltpu.SMEM),
            pl.BlockSpec(memory_space=pltpu.VMEM),
        ]
        + [pl.BlockSpec(memory_space=pltpu.HBM)] * len(arrays),
        scratch_shapes=[
            pltpu.VMEM((parts, units, model), jnp.bfloat16),
            pltpu.SemaphoreType.DMA((model // DOWN_COLUMNS, parts)),
        ],
        compiler_params=pltpu.CompilerParams(vmem_limit_bytes=16 << 20),
        cost_estimate=pl.CostEstimate(
            flops=2 * hidden.size * model, bytes_accessed=6 << 20, transcendentals=0
        ),
        name="down",
    )(flag, hidden, *arrays)


def exchange(rows):
    return lax.all_to_all(rows, "ep", split_axis=0, concat_axis=0, tiled=True)


def layer(
    mixer_input,
    mixer_gain,
    pool_in,
    pool_map,
    pool_scale,
    pool_out,
    expert_input,
    expert_gain,
    group_router,
    expert_router,
    routes,
    gate_weight,
    up_weight,
    down_weight,
):
    tp_count = lax.axis_size("tp")
    tp_place = lax.axis_index("tp")
    experts = expert_router.shape[1]
    block_len = expert_input.shape[0] // tp_count
    slots_each = 4 * block_len // experts

    gates = parts_of(gate_weight[0])
    ups = parts_of(up_weight[0])
    downs = parts_of(down_weight[0])

    toward = jnp.where(lax.axis_index("ep") % 2 == 0, 1, 3)
    starts = [tp_place * block_len, (tp_place ^ toward) * block_len]
    pair_input = jnp.concatenate(
        [lax.dynamic_slice_in_dim(expert_input, start, block_len, 0) for start in starts], axis=0
    )
    pair_routes = jnp.concatenate(
        [lax.dynamic_slice_in_dim(routes, start, block_len, 0) for start in starts], axis=0
    )
    parity = tp_place % 2
    core = jnp.where(jnp.arange(2 * block_len) < block_len, parity, 1 - parity)[:, None]
    targets = jnp.where(pair_routes % 2 == parity, pair_routes - parity + core, -1)
    normed, pick, payload = dispatch(pair_input, expert_gain, targets, experts, slots_each)
    rows = exchange(payload)

    partial_rows = mixer_partial(mixer_input, mixer_gain, pool_in, pool_map, pool_scale, pool_out)
    mixer_output = mixer_reduce(partial_rows)
    weight = route_weights(normed, group_router, expert_router, pair_routes)

    flag = (lax.axis_index("ep") % 2 == parity).astype(jnp.int32).reshape(1)
    hidden = hidden_of(flag, rows, gates, ups)
    result = down_of(
        flag, hidden, downs, jax.ShapeDtypeStruct(payload.shape, jnp.bfloat16)
    )
    returned = exchange(result)
    own, other = combine(returned, pick, weight)
    pairs = [
        (device * tp_count + place, device * tp_count + (place ^ (1 + 2 * (device % 2))))
        for device in range(lax.axis_size("ep"))
        for place in range(tp_count)
    ]
    other = lax.ppermute(other, ("ep", "tp"), pairs)
    expert_output = (own + other.astype(jnp.float32)).astype(jnp.bfloat16)
    return (mixer_output, expert_output)


def solution(mesh):
    return jax.shard_map(
        layer,
        mesh=mesh,
        in_specs=(
            P("ep", None),
            P(),
            P(None, "tp"),
            P("tp", None, None),
            P("tp"),
            P("tp", None),
            P("ep", None),
            P(),
            P(),
            P(),
            P("ep", None),
            P("ep", None, "tp"),
            P("ep", None, "tp"),
            P("ep", "tp", None),
        ),
        out_specs=(P(("ep", "tp"), None), P(("ep", "tp"), None)),
        check_vma=False,
    )
```

```python
import jax
import jax.numpy as jnp
from jax import lax
from jax.experimental import pallas as pl
from jax.experimental.pallas import tpu as pltpu
from jax.sharding import PartitionSpec as P


RIM = 15
EPS = 1e-06


def passed_along(value, axis, steps):
    count = lax.axis_size(axis)
    leading, last = (max(0, -steps), min(count, count - steps))
    return lax.ppermute(value, axis, [(source, source + steps) for source in range(leading, last)])


def swapped(value, mask):
    count = lax.axis_size("tp")
    return lax.ppermute(value, "tp", [(source, source ^ mask) for source in range(count)])


def sent(value, holder_moves, other_moves):
    count = lax.axis_size("tp")
    pairs = []
    for device in range(lax.axis_size("ep")):
        for place in range(count):
            mask, to_holder = holder_moves if device % 2 == place % 2 else other_moves
            goal = place ^ mask
            core = goal % 2 if to_holder else 1 - goal % 2
            pairs.append((device * count + place, (device - device % 2 + core) * count + goal))
    return lax.ppermute(value, ("ep", "tp"), pairs)


def parts_of(own):
    first = sent(own, (0, False), (1, True))
    second = sent(own, (2, False), (3, True))
    first_over = sent(first, (0, False), (0, True))
    second_over = sent(second, (0, False), (0, True))
    return [(own, first), (first, first_over), (second, second_over), (second_over, second)]


def norm_rows(values, gain):
    floats = values.astype(jnp.float32)
    scale = lax.rsqrt(jnp.mean(floats * floats, axis=-1, keepdims=True) + EPS)
    return (floats * scale * gain.astype(jnp.float32)).astype(jnp.bfloat16)


def mixer_partial(mixer_input, mixer_gain, pool_in, pool_map, pool_scale, pool_out):
    normed = norm_rows(mixer_input, mixer_gain)
    pooled_in = jnp.dot(normed, pool_in, preferred_element_type=jnp.float32).astype(jnp.bfloat16)
    local_rows = pooled_in.shape[0]
    groups_here = pool_map.shape[0]
    channels = pool_map.shape[1]
    last = norm_rows(mixer_input[local_rows - RIM - 1 :], mixer_gain)
    last = jnp.dot(last, pool_in, preferred_element_type=jnp.float32).astype(jnp.bfloat16)
    border = passed_along(last[1:], "ep", 1)
    padded = jnp.concatenate([border, pooled_in], axis=0).astype(jnp.float32)
    padded = padded.reshape(local_rows + RIM, groups_here, channels)
    leading = lax.axis_index("tp") * groups_here
    windows = jnp.left_shift(jnp.int32(2), leading + jnp.arange(groups_here, dtype=jnp.int32))
    window_sum = jnp.zeros((local_rows, groups_here, channels), jnp.float32)
    for offset in range(RIM + 1):
        active = (offset < windows).astype(jnp.float32)
        window_sum = (
            window_sum + padded[RIM - offset : RIM - offset + local_rows] * active[None, :, None]
        )
    position = lax.axis_index("ep") * local_rows + jnp.arange(local_rows, dtype=jnp.int32)
    counts_here = jnp.minimum(position[:, None] + 1, windows[None, :]).astype(jnp.float32)
    pooled = (window_sum / counts_here[:, :, None] - padded[RIM:]).astype(jnp.bfloat16)
    mapped = jnp.einsum("tgc,gce->tge", pooled, pool_map, preferred_element_type=jnp.float32)
    mixed_rows = (
        mapped.reshape(local_rows, groups_here * channels) * pool_scale.astype(jnp.float32)
    ).astype(jnp.bfloat16)
    return jnp.dot(mixed_rows, pool_out, preferred_element_type=jnp.float32).astype(jnp.bfloat16)


def mixer_reduce(partial_rows):
    count = lax.axis_size("tp")
    place = lax.axis_index("tp")
    rows = partial_rows.shape[0] // count

    def piece(k):
        return lax.dynamic_slice_in_dim(partial_rows, (place ^ k) * rows, rows, 0)

    total = piece(0).astype(jnp.float32)
    for k in range(1, count):
        part = piece(k)
        total = total + swapped(part, k).astype(jnp.float32)
    return total.astype(jnp.bfloat16)


def dispatch_kernel(x_ref, gain_ref, targets_ref, *outs):
    normed_ref, pick_ref, payload_ref = outs
    tokens = x_ref.shape[0]
    floats = x_ref[...].astype(jnp.float32)
    scale = lax.rsqrt(jnp.mean(floats * floats, axis=-1, keepdims=True) + EPS)
    normed = (floats * scale * gain_ref[...].astype(jnp.float32)).astype(jnp.bfloat16)
    normed_ref[...] = normed
    targets = targets_ref[...]
    slots = pick_ref.shape[2]
    experts = 64
    each = slots // experts
    expert = lax.broadcasted_iota(jnp.int32, (tokens, experts), 1)
    first = targets[:, 0:1] == expert
    second = targets[:, 1:2] == expert
    named = jnp.where(first | second, 1.0, 0.0)
    earlier = lax.broadcasted_iota(jnp.int32, (tokens, tokens), 1) < lax.broadcasted_iota(
        jnp.int32, (tokens, tokens), 0
    )
    before = jnp.dot(
        jnp.where(earlier, 1.0, 0.0).astype(jnp.bfloat16),
        named.astype(jnp.bfloat16),
        preferred_element_type=jnp.float32,
    )
    spread = lax.broadcasted_iota(jnp.int32, (experts, slots), 1) // each == lax.broadcasted_iota(
        jnp.int32, (experts, slots), 0
    )
    spread = jnp.where(spread, 1.0, 0.0).astype(jnp.bfloat16)
    within = (lax.broadcasted_iota(jnp.int32, (tokens, slots), 1) % each).astype(jnp.float32)
    chosen = []
    for mask in (first, second):
        place = jnp.where(mask, before, -1.0).astype(jnp.bfloat16)
        spread_place = jnp.dot(place, spread, preferred_element_type=jnp.float32)
        chosen.append(jnp.where(spread_place == within, 1.0, 0.0))
    pick_ref[0] = chosen[0].astype(jnp.bfloat16)
    pick_ref[1] = chosen[1].astype(jnp.bfloat16)
    either = (chosen[0] + chosen[1]).astype(jnp.bfloat16)
    payload = lax.dot_general(
        either, normed, (((0,), (0,)), ((), ())), preferred_element_type=jnp.float32
    )
    payload_ref[...] = payload.astype(jnp.bfloat16).reshape(payload_ref.shape)


def dispatch(x, gain, targets, experts, slots_each):
    tokens, model = x.shape
    slots = experts * slots_each
    return pl.pallas_call(
        dispatch_kernel,
        out_shape=[
            jax.ShapeDtypeStruct((tokens, model), jnp.bfloat16),
            jax.ShapeDtypeStruct((2, tokens, slots), jnp.bfloat16),
            jax.ShapeDtypeStruct((experts, slots_each // 2, 2, model), jnp.bfloat16),
        ],
        compiler_params=pltpu.CompilerParams(vmem_limit_bytes=16 << 20),
        name="dispatch",
    )(x, gain.reshape(1, model), targets)


def route_weights(rows, group_router, expert_router, route_rows):
    group_logits = jnp.dot(rows, group_router, preferred_element_type=jnp.float32)
    expert_logits = jnp.dot(rows, expert_router, preferred_element_type=jnp.float32)
    groups = group_logits.shape[1]
    experts = expert_logits.shape[1]
    member = (
        jnp.arange(experts, dtype=jnp.int32)[:, None] // (experts // groups)
        == jnp.arange(groups, dtype=jnp.int32)[None, :]
    ).astype(jnp.float32)
    group_exp = jnp.exp(group_logits)
    group_prob = group_exp / jnp.sum(group_exp, axis=1, keepdims=True)
    expert_exp = jnp.exp(expert_logits)
    within = jnp.dot(expert_exp, member, precision=lax.Precision.HIGHEST)
    prob = expert_exp * jnp.dot(group_prob / within, member.T, precision=lax.Precision.HIGHEST)
    chosen = (route_rows[:, :, None] == jnp.arange(experts, dtype=jnp.int32)[None, None, :]).astype(
        jnp.float32
    )
    picked = jnp.sum(chosen * prob[:, None, :], axis=2)
    return picked / jnp.sum(picked, axis=1, keepdims=True)


def combine_kernel(returned_ref, pick_ref, weight_ref, own_ref, other_ref):
    returned = returned_ref[...].reshape(pick_ref.shape[2], returned_ref.shape[-1])
    weight = weight_ref[...]
    total = jnp.dot(pick_ref[0], returned, preferred_element_type=jnp.float32) * weight[:, 0:1]
    total = total + jnp.dot(pick_ref[1], returned, preferred_element_type=jnp.float32) * weight[:, 1:2]
    rows = own_ref.shape[0]
    own_ref[...] = total[:rows]
    other_ref[...] = total[rows:].astype(jnp.bfloat16)


def combine(returned, pick, weight):
    shape = (pick.shape[1] // 2, returned.shape[-1])
    return pl.pallas_call(
        combine_kernel,
        out_shape=[
            jax.ShapeDtypeStruct(shape, jnp.float32),
            jax.ShapeDtypeStruct(shape, jnp.bfloat16),
        ],
        compiler_params=pltpu.CompilerParams(vmem_limit_bytes=12 << 20),
        name="combine",
    )(returned, pick, weight)


def fetch(flag_ref, pair, target, sem):
    @pl.when(flag_ref[0] == 1)
    def _():
        pltpu.make_async_copy(pair[0], target, sem).start()

    @pl.when(flag_ref[0] != 1)
    def _():
        pltpu.make_async_copy(pair[1], target, sem).start()

    return pltpu.make_async_copy(pair[0], target, sem)


def hidden_kernel(flag_ref, rows_ref, *refs):
    out_ref, gate_scratch, up_scratch, sems = refs[-4:]
    count = gate_scratch.shape[0]
    units = gate_scratch.shape[2]

    def start(q):
        pairs = (refs[4 * q], refs[4 * q + 1]), (refs[4 * q + 2], refs[4 * q + 3])
        targets = gate_scratch.at[q], up_scratch.at[q]
        return [fetch(flag_ref, pairs[i], targets[i], sems.at[q, i]) for i in range(2)]

    waits = [start(0), start(1)]
    rows = rows_ref[...].reshape(out_ref.shape[0], rows_ref.shape[-1])
    for q in range(count):
        waits[q][0].wait()
        waits[q][1].wait()
        if q + 2 < count:
            waits.append(start(q + 2))
        gate = jnp.dot(rows, gate_scratch[q], preferred_element_type=jnp.float32)
        up = jnp.dot(rows, up_scratch[q], preferred_element_type=jnp.float32)
        out_ref[:, q * units : (q + 1) * units] = (gate / (1.0 + jnp.exp(-gate)) * up).astype(
            jnp.bfloat16
        )


def hidden_of(flag, rows, gates, ups):
    model, units = gates[0][0].shape
    count = rows.size // model
    parts = len(gates)
    arrays = [array for gate, up in zip(gates, ups) for array in (*gate, *up)]
    return pl.pallas_call(
        hidden_kernel,
        out_shape=jax.ShapeDtypeStruct((count, parts * units), jnp.bfloat16),
        in_specs=[
            pl.BlockSpec(memory_space=pltpu.SMEM),
            pl.BlockSpec(memory_space=pltpu.VMEM),
        ]
        + [pl.BlockSpec(memory_space=pltpu.HBM)] * len(arrays),
        scratch_shapes=[
            pltpu.VMEM((parts, model, units), jnp.bfloat16),
            pltpu.VMEM((parts, model, units), jnp.bfloat16),
            pltpu.SemaphoreType.DMA((parts, 2)),
        ],
        compiler_params=pltpu.CompilerParams(vmem_limit_bytes=58 << 20),
        cost_estimate=pl.CostEstimate(
            flops=4 * count * model * units * parts, bytes_accessed=9 << 20, transcendentals=0
        ),
        name="hidden",
    )(flag, rows, *arrays)


DOWN_COLUMNS = 512


def slot_columns(hidden_ref, flag_ref, on_holder, on_other, units):
    slot = jnp.where(flag_ref[0] == 1, on_holder, on_other)
    return hidden_ref[:, pl.ds(pl.multiple_of(slot * units, units), units)]


def down_near_kernel(flag_ref, hidden_ref, first_ref, second_ref, out_ref):
    units, model = first_ref.shape
    first = slot_columns(hidden_ref, flag_ref, 1, 0, units)
    second = slot_columns(hidden_ref, flag_ref, 2, 3, units)
    for start in range(0, model, DOWN_COLUMNS):
        columns = slice(start, start + DOWN_COLUMNS)
        out_ref[:, columns] = jnp.dot(
            first, first_ref[:, columns], preferred_element_type=jnp.float32
        ) + jnp.dot(second, second_ref[:, columns], preferred_element_type=jnp.float32)


def down_last_kernel(
    flag_ref, hidden_ref, near_ref, second_ref, own_ref, first_ref, out_ref, scratch, sem
):
    units, model = second_ref.shape
    wait = fetch(flag_ref, (own_ref, first_ref), scratch, sem)
    one = slot_columns(hidden_ref, flag_ref, 0, 1, units)
    two = slot_columns(hidden_ref, flag_ref, 3, 2, units)
    wait.wait()
    for start in range(0, model, DOWN_COLUMNS):
        columns = slice(start, start + DOWN_COLUMNS)
        total = jnp.dot(one, scratch[:, columns], preferred_element_type=jnp.float32)
        total = total + jnp.dot(two, second_ref[:, columns], preferred_element_type=jnp.float32)
        total = total + near_ref[:, columns]
        out_ref[:, :, :, columns] = total.astype(jnp.bfloat16).reshape(
            out_ref.shape[:3] + (DOWN_COLUMNS,)
        )


def down_of(flag, hidden, downs, out_shape):
    (own, first), (_, first_over), (second, second_over) = downs[:3]
    units, model = own.shape
    flag_spec = pl.BlockSpec(memory_space=pltpu.SMEM)
    spec = pl.BlockSpec(memory_space=pltpu.VMEM)
    cost = pl.CostEstimate(
        flops=hidden.size * model, bytes_accessed=4 << 20, transcendentals=0
    )
    near = pl.pallas_call(
        down_near_kernel,
        out_shape=jax.ShapeDtypeStruct((hidden.shape[0], model), jnp.float32),
        in_specs=[flag_spec, spec, spec, spec],
        compiler_params=pltpu.CompilerParams(vmem_limit_bytes=16 << 20),
        cost_estimate=cost,
        name="down",
    )(flag, hidden, first, second)
    return pl.pallas_call(
        down_last_kernel,
        out_shape=out_shape,
        in_specs=[flag_spec, spec, spec, spec]
        + [pl.BlockSpec(memory_space=pltpu.HBM)] * 2,
        scratch_shapes=[pltpu.VMEM((units, model), jnp.bfloat16), pltpu.SemaphoreType.DMA],
        compiler_params=pltpu.CompilerParams(vmem_limit_bytes=16 << 20),
        cost_estimate=cost,
        name="down",
    )(flag, hidden, near, second_over, own, first_over)


def exchange(rows):
    return lax.all_to_all(rows, "ep", split_axis=0, concat_axis=0, tiled=True)


def layer(
    mixer_input,
    mixer_gain,
    pool_in,
    pool_map,
    pool_scale,
    pool_out,
    expert_input,
    expert_gain,
    group_router,
    expert_router,
    routes,
    gate_weight,
    up_weight,
    down_weight,
):
    tp_count = lax.axis_size("tp")
    tp_place = lax.axis_index("tp")
    experts = expert_router.shape[1]
    block_len = expert_input.shape[0] // tp_count
    slots_each = 4 * block_len // experts

    gates = parts_of(gate_weight[0])
    ups = parts_of(up_weight[0])
    downs = parts_of(down_weight[0])

    toward = jnp.where(lax.axis_index("ep") % 2 == 0, 1, 3)
    starts = [tp_place * block_len, (tp_place ^ toward) * block_len]
    pair_input = jnp.concatenate(
        [lax.dynamic_slice_in_dim(expert_input, start, block_len, 0) for start in starts], axis=0
    )
    pair_routes = jnp.concatenate(
        [lax.dynamic_slice_in_dim(routes, start, block_len, 0) for start in starts], axis=0
    )
    parity = tp_place % 2
    core = jnp.where(jnp.arange(2 * block_len) < block_len, parity, 1 - parity)[:, None]
    targets = jnp.where(pair_routes % 2 == parity, pair_routes - parity + core, -1)
    normed, pick, payload = dispatch(pair_input, expert_gain, targets, experts, slots_each)
    rows = exchange(payload)

    partial_rows = mixer_partial(mixer_input, mixer_gain, pool_in, pool_map, pool_scale, pool_out)
    mixer_output = mixer_reduce(partial_rows)
    weight = route_weights(normed, group_router, expert_router, pair_routes)

    flag = (lax.axis_index("ep") % 2 == parity).astype(jnp.int32).reshape(1)
    hidden = hidden_of(flag, rows, gates, ups)
    result = down_of(
        flag, hidden, downs, jax.ShapeDtypeStruct(payload.shape, jnp.bfloat16)
    )
    returned = exchange(result)
    own, other = combine(returned, pick, weight)
    pairs = [
        (device * tp_count + place, device * tp_count + (place ^ (1 + 2 * (device % 2))))
        for device in range(lax.axis_size("ep"))
        for place in range(tp_count)
    ]
    other = lax.ppermute(other, ("ep", "tp"), pairs)
    expert_output = (own + other.astype(jnp.float32)).astype(jnp.bfloat16)
    return (mixer_output, expert_output)


def solution(mesh):
    return jax.shard_map(
        layer,
        mesh=mesh,
        in_specs=(
            P("ep", None),
            P(),
            P(None, "tp"),
            P("tp", None, None),
            P("tp"),
            P("tp", None),
            P("ep", None),
            P(),
            P(),
            P(),
            P("ep", None),
            P("ep", None, "tp"),
            P("ep", None, "tp"),
            P("ep", "tp", None),
        ),
        out_specs=(P(("ep", "tp"), None), P(("ep", "tp"), None)),
        check_vma=False,
    )
```

```python
import functools

import jax
import jax.numpy as jnp
from jax import lax
from jax.experimental import pallas as pl
from jax.experimental.pallas import tpu as pltpu
from jax.sharding import PartitionSpec as P


RIM = 15
EPS = 1e-06


def passed_along(value, axis, steps):
    count = lax.axis_size(axis)
    leading, last = (max(0, -steps), min(count, count - steps))
    return lax.ppermute(value, axis, [(source, source + steps) for source in range(leading, last)])


def swapped(value, mask):
    count = lax.axis_size("tp")
    return lax.ppermute(value, "tp", [(source, source ^ mask) for source in range(count)])


def sent(value, holder_moves, other_moves):
    count = lax.axis_size("tp")
    pairs = []
    for device in range(lax.axis_size("ep")):
        for place in range(count):
            mask, to_holder = holder_moves if device % 2 == place % 2 else other_moves
            goal = place ^ mask
            core = goal % 2 if to_holder else 1 - goal % 2
            pairs.append((device * count + place, (device - device % 2 + core) * count + goal))
    return lax.ppermute(value, ("ep", "tp"), pairs)


def parts_of(own):
    first = sent(own, (0, False), (1, True))
    second = sent(own, (2, False), (3, True))
    first_over = sent(first, (0, False), (0, True))
    second_over = sent(second, (0, False), (0, True))
    return [(own, first), (first, first_over), (second, second_over), (second_over, second)]


def norm_rows(values, gain):
    floats = values.astype(jnp.float32)
    scale = lax.rsqrt(jnp.mean(floats * floats, axis=-1, keepdims=True) + EPS)
    return (floats * scale * gain.astype(jnp.float32)).astype(jnp.bfloat16)


def mixer_partial(mixer_input, mixer_gain, pool_in, pool_map, pool_scale, pool_out):
    normed = norm_rows(mixer_input, mixer_gain)
    pooled_in = jnp.dot(normed, pool_in, preferred_element_type=jnp.float32).astype(jnp.bfloat16)
    local_rows = pooled_in.shape[0]
    groups_here = pool_map.shape[0]
    channels = pool_map.shape[1]
    last = norm_rows(mixer_input[local_rows - RIM - 1 :], mixer_gain)
    last = jnp.dot(last, pool_in, preferred_element_type=jnp.float32).astype(jnp.bfloat16)
    border = passed_along(last[1:], "ep", 1)
    padded = jnp.concatenate([border, pooled_in], axis=0).astype(jnp.float32)
    padded = padded.reshape(local_rows + RIM, groups_here, channels)
    leading = lax.axis_index("tp") * groups_here
    windows = jnp.left_shift(jnp.int32(2), leading + jnp.arange(groups_here, dtype=jnp.int32))
    window_sum = jnp.zeros((local_rows, groups_here, channels), jnp.float32)
    for offset in range(RIM + 1):
        active = (offset < windows).astype(jnp.float32)
        window_sum = (
            window_sum + padded[RIM - offset : RIM - offset + local_rows] * active[None, :, None]
        )
    position = lax.axis_index("ep") * local_rows + jnp.arange(local_rows, dtype=jnp.int32)
    counts_here = jnp.minimum(position[:, None] + 1, windows[None, :]).astype(jnp.float32)
    pooled = (window_sum / counts_here[:, :, None] - padded[RIM:]).astype(jnp.bfloat16)
    mapped = jnp.einsum("tgc,gce->tge", pooled, pool_map, preferred_element_type=jnp.float32)
    mixed_rows = (
        mapped.reshape(local_rows, groups_here * channels) * pool_scale.astype(jnp.float32)
    ).astype(jnp.bfloat16)
    return jnp.dot(mixed_rows, pool_out, preferred_element_type=jnp.float32).astype(jnp.bfloat16)


def mixer_reduce(partial_rows):
    count = lax.axis_size("tp")
    place = lax.axis_index("tp")
    rows = partial_rows.shape[0] // count

    def piece(k):
        return lax.dynamic_slice_in_dim(partial_rows, (place ^ k) * rows, rows, 0)

    total = piece(0).astype(jnp.float32)
    for k in range(1, count):
        part = piece(k)
        total = total + swapped(part, k).astype(jnp.float32)
    return total.astype(jnp.bfloat16)


def dispatch_kernel(x_ref, gain_ref, targets_ref, *outs):
    normed_ref, pick_ref, payload_ref = outs
    tokens = x_ref.shape[0]
    floats = x_ref[...].astype(jnp.float32)
    scale = lax.rsqrt(jnp.mean(floats * floats, axis=-1, keepdims=True) + EPS)
    normed = (floats * scale * gain_ref[...].astype(jnp.float32)).astype(jnp.bfloat16)
    normed_ref[...] = normed
    targets = targets_ref[...]
    slots = pick_ref.shape[2]
    experts = 64
    each = slots // experts
    expert = lax.broadcasted_iota(jnp.int32, (tokens, experts), 1)
    first = targets[:, 0:1] == expert
    second = targets[:, 1:2] == expert
    named = jnp.where(first | second, 1.0, 0.0)
    earlier = lax.broadcasted_iota(jnp.int32, (tokens, tokens), 1) < lax.broadcasted_iota(
        jnp.int32, (tokens, tokens), 0
    )
    before = jnp.dot(
        jnp.where(earlier, 1.0, 0.0).astype(jnp.bfloat16),
        named.astype(jnp.bfloat16),
        preferred_element_type=jnp.float32,
    )
    spread = lax.broadcasted_iota(jnp.int32, (experts, slots), 1) // each == lax.broadcasted_iota(
        jnp.int32, (experts, slots), 0
    )
    spread = jnp.where(spread, 1.0, 0.0).astype(jnp.bfloat16)
    within = (lax.broadcasted_iota(jnp.int32, (tokens, slots), 1) % each).astype(jnp.float32)
    chosen = []
    for mask in (first, second):
        place = jnp.where(mask, before, -1.0).astype(jnp.bfloat16)
        spread_place = jnp.dot(place, spread, preferred_element_type=jnp.float32)
        chosen.append(jnp.where(spread_place == within, 1.0, 0.0))
    pick_ref[0] = chosen[0].astype(jnp.bfloat16)
    pick_ref[1] = chosen[1].astype(jnp.bfloat16)
    either = (chosen[0] + chosen[1]).astype(jnp.bfloat16)
    payload = lax.dot_general(
        either, normed, (((0,), (0,)), ((), ())), preferred_element_type=jnp.float32
    )
    payload_ref[...] = payload.astype(jnp.bfloat16).reshape(payload_ref.shape)


def dispatch(x, gain, targets, experts, slots_each):
    tokens, model = x.shape
    slots = experts * slots_each
    return pl.pallas_call(
        dispatch_kernel,
        out_shape=[
            jax.ShapeDtypeStruct((tokens, model), jnp.bfloat16),
            jax.ShapeDtypeStruct((2, tokens, slots), jnp.bfloat16),
            jax.ShapeDtypeStruct((experts, slots_each // 2, 2, model), jnp.bfloat16),
        ],
        compiler_params=pltpu.CompilerParams(vmem_limit_bytes=16 << 20),
        name="dispatch",
    )(x, gain.reshape(1, model), targets)


def route_weights(rows, group_router, expert_router, route_rows):
    group_logits = jnp.dot(rows, group_router, preferred_element_type=jnp.float32)
    expert_logits = jnp.dot(rows, expert_router, preferred_element_type=jnp.float32)
    groups = group_logits.shape[1]
    experts = expert_logits.shape[1]
    member = (
        jnp.arange(experts, dtype=jnp.int32)[:, None] // (experts // groups)
        == jnp.arange(groups, dtype=jnp.int32)[None, :]
    ).astype(jnp.float32)
    group_exp = jnp.exp(group_logits)
    group_prob = group_exp / jnp.sum(group_exp, axis=1, keepdims=True)
    expert_exp = jnp.exp(expert_logits)
    within = jnp.dot(expert_exp, member, precision=lax.Precision.HIGHEST)
    prob = expert_exp * jnp.dot(group_prob / within, member.T, precision=lax.Precision.HIGHEST)
    chosen = (route_rows[:, :, None] == jnp.arange(experts, dtype=jnp.int32)[None, None, :]).astype(
        jnp.float32
    )
    picked = jnp.sum(chosen * prob[:, None, :], axis=2)
    return picked / jnp.sum(picked, axis=1, keepdims=True)


def combine_kernel(first_row, returned_ref, pick_ref, weight_ref, out_ref):
    returned = returned_ref[...].reshape(pick_ref.shape[2], returned_ref.shape[-1])
    rows = slice(first_row, first_row + out_ref.shape[0])
    weight = weight_ref[rows, :]
    total = jnp.dot(pick_ref[0, rows, :], returned, preferred_element_type=jnp.float32)
    total = total * weight[:, 0:1]
    second = jnp.dot(pick_ref[1, rows, :], returned, preferred_element_type=jnp.float32)
    out_ref[...] = (total + second * weight[:, 1:2]).astype(out_ref.dtype)


def combine(returned, pick, weight, block, dtype):
    rows = pick.shape[1] // 2
    return pl.pallas_call(
        functools.partial(combine_kernel, block * rows),
        out_shape=jax.ShapeDtypeStruct((rows, returned.shape[-1]), dtype),
        compiler_params=pltpu.CompilerParams(vmem_limit_bytes=12 << 20),
        name="combine",
    )(returned, pick, weight)


def fetch(flag_ref, pair, target, sem):
    @pl.when(flag_ref[0] == 1)
    def _():
        pltpu.make_async_copy(pair[0], target, sem).start()

    @pl.when(flag_ref[0] != 1)
    def _():
        pltpu.make_async_copy(pair[1], target, sem).start()

    return pltpu.make_async_copy(pair[0], target, sem)


def hidden_kernel(flag_ref, rows_ref, *refs):
    out_ref, gate_scratch, up_scratch, sems = refs[-4:]
    count = gate_scratch.shape[0]
    units = gate_scratch.shape[2]

    def start(q):
        pairs = (refs[4 * q], refs[4 * q + 1]), (refs[4 * q + 2], refs[4 * q + 3])
        targets = gate_scratch.at[q], up_scratch.at[q]
        return [fetch(flag_ref, pairs[i], targets[i], sems.at[q, i]) for i in range(2)]

    waits = [start(0), start(1)]
    rows = rows_ref[...].reshape(out_ref.shape[0], rows_ref.shape[-1])
    for q in range(count):
        waits[q][0].wait()
        waits[q][1].wait()
        if q + 2 < count:
            waits.append(start(q + 2))
        gate = jnp.dot(rows, gate_scratch[q], preferred_element_type=jnp.float32)
        up = jnp.dot(rows, up_scratch[q], preferred_element_type=jnp.float32)
        out_ref[:, q * units : (q + 1) * units] = (gate / (1.0 + jnp.exp(-gate)) * up).astype(
            jnp.bfloat16
        )


def hidden_of(flag, rows, gates, ups):
    model, units = gates[0][0].shape
    count = rows.size // model
    parts = len(gates)
    arrays = [array for gate, up in zip(gates, ups) for array in (*gate, *up)]
    return pl.pallas_call(
        hidden_kernel,
        out_shape=jax.ShapeDtypeStruct((count, parts * units), jnp.bfloat16),
        in_specs=[
            pl.BlockSpec(memory_space=pltpu.SMEM),
            pl.BlockSpec(memory_space=pltpu.VMEM),
        ]
        + [pl.BlockSpec(memory_space=pltpu.HBM)] * len(arrays),
        scratch_shapes=[
            pltpu.VMEM((parts, model, units), jnp.bfloat16),
            pltpu.VMEM((parts, model, units), jnp.bfloat16),
            pltpu.SemaphoreType.DMA((parts, 2)),
        ],
        compiler_params=pltpu.CompilerParams(vmem_limit_bytes=58 << 20),
        cost_estimate=pl.CostEstimate(
            flops=4 * count * model * units * parts, bytes_accessed=9 << 20, transcendentals=0
        ),
        name="hidden",
    )(flag, rows, *arrays)


DOWN_COLUMNS = 512


def slot_columns(hidden_ref, flag_ref, on_holder, on_other, units):
    slot = jnp.where(flag_ref[0] == 1, on_holder, on_other)
    return hidden_ref[:, pl.ds(pl.multiple_of(slot * units, units), units)]


def down_near_kernel(flag_ref, hidden_ref, first_ref, second_ref, out_ref):
    units, model = first_ref.shape
    first = slot_columns(hidden_ref, flag_ref, 1, 0, units)
    second = slot_columns(hidden_ref, flag_ref, 2, 3, units)
    for start in range(0, model, DOWN_COLUMNS):
        columns = slice(start, start + DOWN_COLUMNS)
        out_ref[:, columns] = jnp.dot(
            first, first_ref[:, columns], preferred_element_type=jnp.float32
        ) + jnp.dot(second, second_ref[:, columns], preferred_element_type=jnp.float32)


def down_last_kernel(
    flag_ref, hidden_ref, near_ref, second_ref, own_ref, first_ref, out_ref, scratch, sem
):
    units, model = second_ref.shape
    wait = fetch(flag_ref, (own_ref, first_ref), scratch, sem)
    one = slot_columns(hidden_ref, flag_ref, 0, 1, units)
    two = slot_columns(hidden_ref, flag_ref, 3, 2, units)
    wait.wait()
    for start in range(0, model, DOWN_COLUMNS):
        columns = slice(start, start + DOWN_COLUMNS)
        total = jnp.dot(one, scratch[:, columns], preferred_element_type=jnp.float32)
        total = total + jnp.dot(two, second_ref[:, columns], preferred_element_type=jnp.float32)
        total = total + near_ref[:, columns]
        out_ref[:, :, :, columns] = total.astype(jnp.bfloat16).reshape(
            out_ref.shape[:3] + (DOWN_COLUMNS,)
        )


def down_of(flag, hidden, downs, out_shape):
    (own, first), (_, first_over), (second, second_over) = downs[:3]
    units, model = own.shape
    flag_spec = pl.BlockSpec(memory_space=pltpu.SMEM)
    spec = pl.BlockSpec(memory_space=pltpu.VMEM)
    cost = pl.CostEstimate(
        flops=hidden.size * model, bytes_accessed=4 << 20, transcendentals=0
    )
    near = pl.pallas_call(
        down_near_kernel,
        out_shape=jax.ShapeDtypeStruct((hidden.shape[0], model), jnp.float32),
        in_specs=[flag_spec, spec, spec, spec],
        compiler_params=pltpu.CompilerParams(vmem_limit_bytes=16 << 20),
        cost_estimate=cost,
        name="down",
    )(flag, hidden, first, second)
    return pl.pallas_call(
        down_last_kernel,
        out_shape=out_shape,
        in_specs=[flag_spec, spec, spec, spec]
        + [pl.BlockSpec(memory_space=pltpu.HBM)] * 2,
        scratch_shapes=[pltpu.VMEM((units, model), jnp.bfloat16), pltpu.SemaphoreType.DMA],
        compiler_params=pltpu.CompilerParams(vmem_limit_bytes=16 << 20),
        cost_estimate=cost,
        name="down",
    )(flag, hidden, near, second_over, own, first_over)


def exchange(rows):
    return lax.all_to_all(rows, "ep", split_axis=0, concat_axis=0, tiled=True)


def layer(
    mixer_input,
    mixer_gain,
    pool_in,
    pool_map,
    pool_scale,
    pool_out,
    expert_input,
    expert_gain,
    group_router,
    expert_router,
    routes,
    gate_weight,
    up_weight,
    down_weight,
):
    tp_count = lax.axis_size("tp")
    tp_place = lax.axis_index("tp")
    experts = expert_router.shape[1]
    block_len = expert_input.shape[0] // tp_count
    slots_each = 4 * block_len // experts

    gates = parts_of(gate_weight[0])
    ups = parts_of(up_weight[0])
    downs = parts_of(down_weight[0])

    toward = jnp.where(lax.axis_index("ep") % 2 == 0, 1, 3)
    starts = [tp_place * block_len, (tp_place ^ toward) * block_len]
    pair_input = jnp.concatenate(
        [lax.dynamic_slice_in_dim(expert_input, start, block_len, 0) for start in starts], axis=0
    )
    pair_routes = jnp.concatenate(
        [lax.dynamic_slice_in_dim(routes, start, block_len, 0) for start in starts], axis=0
    )
    parity = tp_place % 2
    core = jnp.where(jnp.arange(2 * block_len) < block_len, parity, 1 - parity)[:, None]
    targets = jnp.where(pair_routes % 2 == parity, pair_routes - parity + core, -1)
    normed, pick, payload = dispatch(pair_input, expert_gain, targets, experts, slots_each)
    rows = exchange(payload)

    partial_rows = mixer_partial(mixer_input, mixer_gain, pool_in, pool_map, pool_scale, pool_out)
    mixer_output = mixer_reduce(partial_rows)
    weight = route_weights(normed, group_router, expert_router, pair_routes)

    flag = (lax.axis_index("ep") % 2 == parity).astype(jnp.int32).reshape(1)
    hidden = hidden_of(flag, rows, gates, ups)
    result = down_of(
        flag, hidden, downs, jax.ShapeDtypeStruct(payload.shape, jnp.bfloat16)
    )
    returned = exchange(result)
    other = combine(returned, pick, weight, 1, jnp.bfloat16)
    own = combine(returned, pick, weight, 0, jnp.float32)
    pairs = [
        (device * tp_count + place, device * tp_count + (place ^ (1 + 2 * (device % 2))))
        for device in range(lax.axis_size("ep"))
        for place in range(tp_count)
    ]
    other = lax.ppermute(other, ("ep", "tp"), pairs)
    expert_output = (own + other.astype(jnp.float32)).astype(jnp.bfloat16)
    return (mixer_output, expert_output)


def solution(mesh):
    return jax.shard_map(
        layer,
        mesh=mesh,
        in_specs=(
            P("ep", None),
            P(),
            P(None, "tp"),
            P("tp", None, None),
            P("tp"),
            P("tp", None),
            P("ep", None),
            P(),
            P(),
            P(),
            P("ep", None),
            P("ep", None, "tp"),
            P("ep", None, "tp"),
            P("ep", "tp", None),
        ),
        out_specs=(P(("ep", "tp"), None), P(("ep", "tp"), None)),
        check_vma=False,
    )
```
